32 devices in a mesh: kv: 16 (over z, y, x), tp: 2 (over core).
Axes of the slice: x: 2, y: 2, z: 4, core: 2. Of those that a mesh axis runs over, the one named last changes fastest.
Arguments:
- tokens: bfloat16 [4, 4, 4096], replicated, may hold values from -6 to 6
- parents: int32 [4, 4], replicated, may hold values from -1 to 2, as said below
- lengths: int32 [4], replicated, may hold values from 1 to 2040, as said below
- accepted: int32 [4], replicated, may hold values from 0 to 4
- in_gain: float32 [4096], replicated, may hold values from 0.1 to 1.9
- w_query: bfloat16 [4096, 3072], P('kv', 'tp'), may hold values from -0.09375 to 0.09375
- w_latent: bfloat16 [4096, 1024], P('kv'), may hold values from -0.09375 to 0.09375
- w_rope_key: bfloat16 [4096, 32], replicated, may hold values from -0.09375 to 0.09375
- latent_gain: float32 [1024], replicated, may hold values from 0.1 to 1.9
- query_gain: float32 [96], replicated, may hold values from 0.4 to 160, as said below
- key_gain: float32 [96], replicated, may hold values from 0.1 to 1.9
- w_key_up: bfloat16 [1024, 2048], P(None, 'tp'), may hold values from -0.1875 to 0.1875
- w_value_up: bfloat16 [1024, 2048], P(None, 'tp'), may hold values from -0.1875 to 0.1875
- w_out: bfloat16 [2048, 4096], P('tp', 'kv'), may hold values from -1 to 1
- out_gain: float32 [4096], P('kv'), may hold values from 0.1 to 1.9
- cache_latent: bfloat16 [4, 2048, 1024], P(None, 'kv'), may hold values from -6 to 6
- cache_rope: bfloat16 [4, 2048, 32], P(None, 'kv'), may hold values from -6 to 6
Outputs:
- mixed: bfloat16 [4, 4, 4096], P(None, None, 'kv')
- new_latent: bfloat16 [4, 2048, 1024], P(None, 'kv')
- new_rope: bfloat16 [4, 2048, 32], P(None, 'kv')
The draws below stay inside these ranges and needn't reach their ends.
Inputs may be any that keep to these rules, and one draw needn't show every extreme that they name: parents[s, 0] is -1; for i of 1 or more parents[s, i] lies in 0 to i - 1. `lengths`: the first sequence's length is at most 8, the last one's at least 1912. `query_gain`: positive.
All inputs are finite; a program needn't handle non-finite values.
Results may differ from the reference program's by a relative error of at most 0.008.
The reference program's roundings to bfloat16 on the way count: a program that leaves them out, or rounds other values in their place, can miss the bound.
Values sent between devices are 32-bit elements; how exact they have to be, the bound alone decides.
A program may use at most 64 MiB of HBM per device.

```python
import jax
import jax.numpy as jnp
from jax import lax

D = 4096
HEADS = 32
NOPE = 64
ROPE = 32
QK = 96
VDIM = 64
LATENT = 1024
SEQS = 4
PROPS = 4
POS_DEV = 128
CACHE_LEN = 2048


def draw_parents(key, part):
    raw_bits = jax.random.randint(jax.random.fold_in(key, 11), (SEQS, PROPS), 0, 1 << 20)
    indices = jnp.arange(PROPS, dtype=jnp.int32)
    chosen = raw_bits % jnp.maximum(indices, 1)[None, :]
    return jnp.where(indices[None, :] == 0, -1, chosen).astype(jnp.int32)


def draw_lengths(key, part):
    key_short, key_edge, key_backward, key_last = jax.random.split(jax.random.fold_in(key, 23), 4)
    short_len = jax.random.randint(key_short, (1,), 1, 2 * PROPS + 1)
    blocks = jax.random.randint(key_edge, (SEQS - 2,), 1, CACHE_LEN // POS_DEV)
    backward = jax.random.randint(key_backward, (SEQS - 2,), 1, PROPS + 1)
    middle = blocks * POS_DEV - backward
    last_len = jax.random.randint(key_last, (1,), CACHE_LEN - POS_DEV - 2 * PROPS, CACHE_LEN - 2 * PROPS + 1)
    return jnp.concatenate([short_len, middle, last_len]).astype(jnp.int32)


def draw_query_gain(key, part):
    key_noise = jax.random.fold_in(jax.random.fold_in(key, 37), 0)
    key_pick = jax.random.fold_in(jax.random.fold_in(key, 37), 2)
    order = jax.random.permutation(key_pick, NOPE)
    dims = jnp.arange(QK, dtype=jnp.int32)
    strong = (dims == order[0]) | (dims == order[1])
    noise = jax.random.normal(key_noise, (QK,), jnp.float32)
    base = jnp.exp(0.3 * jnp.clip(noise, -3.0, 3.0))
    return jnp.where(strong, 100.0, base).astype(jnp.float32)


def draw_w_out(key, part):
    key_entries, key_columns = jax.random.split(jax.random.fold_in(key, 41))
    fraction = jnp.arange(D, dtype=jnp.float32) / D
    jitter = jnp.exp(jax.random.uniform(key_columns, (D,), jnp.float32, -0.7, 0.7))
    entries = jnp.clip(jax.random.normal(key_entries, (HEADS * VDIM, D), jnp.float32), -5.0, 5.0)
    column_scale = 10.0 ** (fraction - 0.5) * jitter
    return (entries * column_scale[None, :] * (HEADS * VDIM) ** (-0.5)).astype(jnp.bfloat16)


def touch_ends(drawn, key, least, top_value):
    longest = drawn.shape.index(max(drawn.shape))
    spots = []
    for shift in (0, 1):
        where = [jax.random.randint(jax.random.fold_in(key, axis), (), 0, length) for axis, length in enumerate(drawn.shape)]
        where[longest] = (where[longest] + shift) % drawn.shape[longest]
        spots.append(tuple(where))
    return drawn.at[spots[0]].set(least).at[spots[1]].set(top_value)


def levels(stream_key, shape, cuts, low, top_value):
    factor_of = 1.0
    for dim, parts in cuts:
        steps = jax.random.uniform(jax.random.fold_in(jax.random.fold_in(stream_key, 6), dim), (parts,), jnp.float32, low / len(cuts), top_value / len(cuts))
        factor_of = factor_of * jnp.repeat(jnp.exp(steps), shape[dim] // parts).reshape((-1,) + (1,) * (len(shape) - 1 - dim))
    return factor_of


def normal_values(stream_key, shape, scale, reach, pieces=(), kind=jnp.bfloat16):
    gain = levels(stream_key, shape, pieces, -0.22, 0.18) if pieces else 1.0
    values = jax.random.normal(stream_key, shape, jnp.float32) * scale * gain
    return jnp.minimum(jnp.maximum(values, -reach), reach).astype(kind)


def setup_inputs(seed: int = 0) -> dict:
    streams_of = jax.random.split(jax.random.key(seed), 18)
    return {
        "tokens": normal_values(streams_of[0], (SEQS, PROPS, D), 1.0, 6.0),
        "parents": draw_parents(jax.random.fold_in(streams_of[17], 71), 0),
        "lengths": draw_lengths(jax.random.fold_in(streams_of[17], 71), 0),
        "accepted": touch_ends(jax.random.randint(streams_of[3], (SEQS,), 0, PROPS + 1), jax.random.fold_in(streams_of[3], 1), 0, PROPS).astype(jnp.int32),
        "in_gain": jnp.clip(1.0 + 0.18 * jax.random.normal(streams_of[4], (D,), jnp.float32), 0.1, 1.9),
        "w_query": normal_values(streams_of[5], (D, HEADS * QK), D ** -0.5, 0.09375, ((0, 16), (1, 2))),
        "w_latent": normal_values(streams_of[6], (D, LATENT), D ** -0.5, 0.09375, ((0, 16),)),
        "w_rope_key": normal_values(streams_of[7], (D, ROPE), D ** -0.5, 0.09375),
        "latent_gain": jnp.clip(1.0 + 0.18 * jax.random.normal(streams_of[8], (LATENT,), jnp.float32), 0.1, 1.9),
        "query_gain": draw_query_gain(jax.random.fold_in(streams_of[17], 71), 0),
        "key_gain": jnp.clip(1.0 + 0.18 * jax.random.normal(streams_of[10], (QK,), jnp.float32), 0.1, 1.9),
        "w_key_up": normal_values(streams_of[11], (LATENT, HEADS * NOPE), LATENT ** -0.5, 0.1875, ((1, 2),)),
        "w_value_up": normal_values(streams_of[12], (LATENT, HEADS * VDIM), LATENT ** -0.5, 0.1875, ((1, 2),)),
        "w_out": draw_w_out(jax.random.fold_in(streams_of[17], 71), 0),
        "out_gain": jnp.clip(1.0 + 0.18 * jax.random.normal(streams_of[14], (D,), jnp.float32), 0.1, 1.9),
        "cache_latent": normal_values(streams_of[15], (SEQS, CACHE_LEN, LATENT), 1.0, 6.0, ((1, 16),)),
        "cache_rope": normal_values(streams_of[16], (SEQS, CACHE_LEN, ROPE), 1.0, 6.0, ((1, 16),)),
    }


epsilon = 1e-06
rope_base = 10000.0

def ancestry(parents):
    prop_count = parents.shape[-1]
    indices = jnp.arange(prop_count, dtype=jnp.int32)
    step_map = (parents[..., :, None] == indices).astype(jnp.int32)
    identity_map = jnp.broadcast_to((indices[:, None] == indices[None, :]).astype(jnp.int32), step_map.shape)
    reached = identity_map
    hop_map = identity_map
    for step_index in range(prop_count - 1):
        hop_map = jnp.einsum('sij,sjk->sik', hop_map, step_map)
        reached = reached + hop_map
    return reached

def angles(positions):
    halfway = ROPE // 2
    inverse = rope_base ** (-jnp.arange(halfway, dtype=jnp.float32) / halfway)
    angle = positions.astype(jnp.float32)[..., None] * inverse
    return (jnp.cos(angle), jnp.sin(angle))

def rotate(vectors, cosine, sine_part):
    halfway = vectors.shape[-1] // 2
    leading = vectors[..., :halfway]
    trailing = vectors[..., halfway:]
    return jnp.concatenate([leading * cosine - trailing * sine_part, trailing * cosine + leading * sine_part], -1)

def keys_of(latents, rope_rows, w_key_up, key_gain):
    row_count = latents.shape[0]
    nope = jnp.dot(latents, w_key_up, preferred_element_type=jnp.float32).reshape(row_count, HEADS, NOPE)
    rope_wide = jnp.broadcast_to(rope_rows.astype(jnp.float32)[:, None, :], (row_count, HEADS, ROPE))
    joined = jnp.concatenate([nope, rope_wide], -1)
    factor = lax.rsqrt(lax.optimization_barrier(jnp.mean(joined * joined, -1, keepdims=True)) + epsilon)
    return (joined * factor * key_gain).astype(jnp.bfloat16)

def reference(tokens, parents, lengths, accepted, in_gain, w_query, w_latent, w_rope_key, latent_gain, query_gain, key_gain, w_key_up, w_value_up, w_out, out_gain, cache_latent, cache_rope):
    row_count = SEQS * PROPS
    flattened = tokens.reshape(row_count, D).astype(jnp.float32)
    normed = (flattened * lax.rsqrt(lax.optimization_barrier(jnp.mean(flattened * flattened, -1, keepdims=True)) + epsilon) * in_gain).astype(jnp.bfloat16)
    query_raw = jnp.dot(normed, w_query, preferred_element_type=jnp.float32).reshape(SEQS, PROPS, HEADS, QK)
    latent_raw = jnp.dot(normed, w_latent, preferred_element_type=jnp.float32).reshape(SEQS, PROPS, LATENT)
    rope_raw = jnp.dot(normed, w_rope_key, preferred_element_type=jnp.float32).reshape(SEQS, PROPS, ROPE)
    reached = ancestry(parents)
    anchor = (lengths + accepted).astype(jnp.int32)
    positions = anchor[:, None] + lax.optimization_barrier(jnp.sum(reached, -1)) - 1
    cosine, sine_part = angles(positions)
    turned = rotate(query_raw[..., NOPE:], cosine[:, :, None, :], sine_part[:, :, None, :])
    joined = jnp.concatenate([query_raw[..., :NOPE], turned], -1)
    query = (joined * lax.rsqrt(lax.optimization_barrier(jnp.mean(joined * joined, -1, keepdims=True)) + epsilon) * query_gain).astype(jnp.bfloat16)
    latent_new = (latent_raw * lax.rsqrt(lax.optimization_barrier(jnp.mean(latent_raw * latent_raw, -1, keepdims=True)) + epsilon) * latent_gain).astype(jnp.bfloat16)
    rope_new = rotate(rope_raw, cosine, sine_part).astype(jnp.bfloat16)

    def place(table, fresh, start):
        return lax.dynamic_update_slice(table, fresh, (start.astype(jnp.int32), jnp.zeros((), jnp.int32)))
    new_latent = jax.vmap(place)(cache_latent, latent_new, anchor)
    new_rope = jax.vmap(place)(cache_rope, rope_new, anchor)
    score_scale = QK ** (-0.5)

    def attend_one(inputs):
        query_s, latent_s, rope_s, reached_s, anchor_s, cache_lat, cache_rot = inputs
        keys_cache = keys_of(cache_lat, cache_rot, w_key_up, key_gain)
        keys_own = keys_of(latent_s, rope_s, w_key_up, key_gain)
        query_f = query_s.astype(jnp.float32)
        scores_cache = jnp.einsum('phd,lhd->hpl', query_f, keys_cache.astype(jnp.float32)) * score_scale
        visible = jnp.arange(cache_lat.shape[0], dtype=jnp.int32) < anchor_s
        scores_cache = jnp.where(visible[None, None, :], scores_cache, -jnp.inf)
        scores_own = jnp.einsum('phd,khd->hpk', query_f, keys_own.astype(jnp.float32)) * score_scale
        scores_own = jnp.where(reached_s[None] > 0, scores_own, -jnp.inf)
        highest = jnp.maximum(lax.optimization_barrier(jnp.max(scores_cache, -1)), lax.optimization_barrier(jnp.max(scores_own, -1)))
        weights_cache = jnp.exp(scores_cache - highest[..., None])
        weights_own = jnp.exp(scores_own - highest[..., None])
        totals = lax.optimization_barrier(jnp.sum(weights_cache, -1)) + lax.optimization_barrier(jnp.sum(weights_own, -1))
        summed = jnp.einsum('hpl,lc->phc', weights_cache.astype(jnp.bfloat16).astype(jnp.float32), cache_lat.astype(jnp.float32))
        summed = summed + jnp.einsum('hpk,kc->phc', weights_own.astype(jnp.bfloat16).astype(jnp.float32), latent_s.astype(jnp.float32))
        return summed / jnp.transpose(totals)[..., None]
    attended = lax.map(attend_one, (query, latent_new, rope_new, reached, anchor, cache_latent, cache_rope))
    value_up = w_value_up.astype(jnp.float32).reshape(LATENT, HEADS, VDIM)
    values = jnp.einsum('sphc,chd->sphd', attended, value_up, precision=lax.Precision.HIGHEST)
    values_low = values.astype(jnp.bfloat16).reshape(row_count, HEADS * VDIM)
    projected = jnp.dot(values_low, w_out, preferred_element_type=jnp.float32)
    mixed = (projected * lax.rsqrt(lax.optimization_barrier(jnp.mean(projected * projected, -1, keepdims=True)) + epsilon) * out_gain).astype(jnp.bfloat16)
    return (mixed.reshape(SEQS, PROPS, D), new_latent, new_rope)
```

```python
import functools

import jax
import jax.numpy as jnp
import numpy as np
from jax import lax
from jax.experimental import pallas as pl
from jax.experimental.pallas import tpu as pltpu
from jax.sharding import PartitionSpec as P

MESH = pl.DeviceIdType.MESH

D = 4096
NOPE = 64
ROPE = 32
QK = 96
VDIM = 64


epsilon = 1e-06
rope_base = 10000.0


def combined_all(value, axis, join):
    pieces = jax.tree.map(lambda part: lax.all_gather(part, axis), value)
    head = jax.tree.map(lambda part: part[0], pieces)
    tail = jax.tree.map(lambda part: part[1:], pieces)
    running, _ = lax.scan(lambda running, piece: (join(running, piece), None), head, tail)
    return running


def ancestry(parents):
    prop_count = parents.shape[-1]
    indices = jnp.arange(prop_count, dtype=jnp.int32)
    step_map = (parents[..., :, None] == indices).astype(jnp.int32)
    identity_map = jnp.broadcast_to(
        (indices[:, None] == indices[None, :]).astype(jnp.int32), step_map.shape
    )
    reached = identity_map
    hop_map = identity_map
    for step_index in range(prop_count - 1):
        hop_map = jnp.einsum("sij,sjk->sik", hop_map, step_map)
        reached = reached + hop_map
    return reached


def angles(positions):
    halfway = ROPE // 2
    inverse = rope_base ** (-jnp.arange(halfway, dtype=jnp.float32) / halfway)
    angle = positions.astype(jnp.float32)[..., None] * inverse
    return (jnp.cos(angle), jnp.sin(angle))


def rotate(vectors, cosine, sine_part):
    halfway = vectors.shape[-1] // 2
    leading = vectors[..., :halfway]
    trailing = vectors[..., halfway:]
    return jnp.concatenate(
        [leading * cosine - trailing * sine_part, trailing * cosine + leading * sine_part], -1
    )


def split_keys(latents, rope_rows, w_key_up, key_gain):
    head_count = w_key_up.shape[1] // NOPE
    nope = jnp.dot(latents, w_key_up, preferred_element_type=jnp.float32)
    nope = nope.reshape(latents.shape[:2] + (head_count, NOPE))
    rope_wide = rope_rows.astype(jnp.float32)[:, :, None, :]
    squares = jnp.sum(nope * nope, -1) + jnp.sum(rope_wide * rope_wide, -1)
    factor = lax.rsqrt(squares / QK + epsilon)[..., None]
    key_nope = (nope * factor * key_gain[:NOPE]).astype(jnp.bfloat16)
    key_rope = (rope_wide * factor * key_gain[NOPE:]).astype(jnp.bfloat16)
    return (key_nope, key_rope)


def attend_block(query, key_nope, key_rope, latents, visible):
    score_scale = QK ** (-0.5)
    scores = jnp.einsum(
        "sphd,slhd->shpl", query[..., :NOPE], key_nope, preferred_element_type=jnp.float32
    )
    scores = scores + jnp.einsum(
        "sphd,slhd->shpl", query[..., NOPE:], key_rope, preferred_element_type=jnp.float32
    )
    scores = jnp.where(visible, scores * score_scale, -1e30)
    peaks = jnp.max(scores, -1)
    weights = jnp.where(visible, jnp.exp(scores - peaks[..., None]), 0.0)
    totals = jnp.sum(weights, -1)
    summed = jnp.einsum(
        "shpl,slc->sphc", weights.astype(jnp.bfloat16), latents, preferred_element_type=jnp.float32
    )
    return (jnp.swapaxes(peaks, 1, 2), jnp.swapaxes(totals, 1, 2), summed)


def combine(left_part, right_part):
    left_peak, left_total, left_sum = left_part
    right_peak, right_total, right_sum = right_part
    highest = jnp.maximum(left_peak, right_peak)
    left_scale = jnp.exp(left_peak - highest)
    right_scale = jnp.exp(right_peak - highest)
    return (
        highest,
        left_total * left_scale + right_total * right_scale,
        left_sum * left_scale[..., None] + right_sum * right_scale[..., None],
    )


def body(
    tokens,
    parents,
    lengths,
    accepted,
    in_gain,
    w_query,
    w_latent,
    w_rope_key,
    latent_gain,
    query_gain,
    key_gain,
    w_key_up,
    w_value_up,
    w_out,
    out_gain,
    cache_latent,
    cache_rope,
):
    seq_count, prop_count, model_width = tokens.shape
    row_count = seq_count * prop_count
    head_count = w_key_up.shape[1] // NOPE
    flattened = tokens.reshape(row_count, model_width).astype(jnp.float32)
    normed = (
        flattened
        * lax.rsqrt(jnp.mean(flattened * flattened, -1, keepdims=True) + epsilon)
        * in_gain
    ).astype(jnp.bfloat16)
    part_rows = w_query.shape[0]
    normed_part = lax.dynamic_slice_in_dim(normed, lax.axis_index("kv") * part_rows, part_rows, 1)
    query_part = jnp.dot(normed_part, w_query, preferred_element_type=jnp.float32)
    latent_part = jnp.dot(normed_part, w_latent, preferred_element_type=jnp.float32)
    query_raw, latent_raw = lax.psum((query_part, latent_part), "kv")
    rope_raw = jnp.dot(normed, w_rope_key, preferred_element_type=jnp.float32).reshape(
        seq_count, prop_count, ROPE
    )
    latent_raw = latent_raw.reshape(seq_count, prop_count, -1)
    reached = ancestry(parents)
    anchor = lengths + accepted
    positions = anchor[:, None] + jnp.sum(reached, -1) - 1
    cosine, sine_part = angles(positions)
    query_raw = query_raw.reshape(seq_count, prop_count, head_count, QK)
    turned = rotate(query_raw[..., NOPE:], cosine[:, :, None, :], sine_part[:, :, None, :])
    joined = jnp.concatenate([query_raw[..., :NOPE], turned], -1)
    query = (
        joined * lax.rsqrt(jnp.mean(joined * joined, -1, keepdims=True) + epsilon) * query_gain
    ).astype(jnp.bfloat16)
    latent_new = (
        latent_raw
        * lax.rsqrt(jnp.mean(latent_raw * latent_raw, -1, keepdims=True) + epsilon)
        * latent_gain
    ).astype(jnp.bfloat16)
    rope_new = rotate(rope_raw, cosine, sine_part).astype(jnp.bfloat16)
    shard_len = cache_latent.shape[1]
    places = lax.axis_index("kv") * shard_len + jnp.arange(shard_len, dtype=jnp.int32)
    offset = places[None, :] - anchor[:, None]
    selected = offset[:, :, None] == jnp.arange(prop_count, dtype=jnp.int32)[None, None, :]
    filled = jnp.any(selected, -1)[..., None]
    selector = selected.astype(jnp.bfloat16)
    placed_latent = jnp.einsum(
        "slp,spc->slc", selector, latent_new, preferred_element_type=jnp.float32
    ).astype(jnp.bfloat16)
    placed_rope = jnp.einsum(
        "slp,spc->slc", selector, rope_new, preferred_element_type=jnp.float32
    ).astype(jnp.bfloat16)
    new_latent = jnp.where(filled, placed_latent, cache_latent)
    new_rope = jnp.where(filled, placed_rope, cache_rope)
    key_nope, key_rope = split_keys(cache_latent, cache_rope, w_key_up, key_gain)
    cache_seen = (places[None, :] < anchor[:, None])[:, None, None, :]
    block_peak, block_total, block_sum = attend_block(
        query, key_nope, key_rope, cache_latent, cache_seen
    )
    own_nope, own_rope = split_keys(latent_new, rope_new, w_key_up, key_gain)
    own_seen = (reached > 0)[:, None, :, :]
    own_peak, own_total, own_sum = attend_block(query, own_nope, own_rope, latent_new, own_seen)
    value_up = w_value_up.astype(jnp.float32).reshape(w_value_up.shape[0], head_count, VDIM)

    def to_values(summed):
        return jnp.einsum("sphc,chd->sphd", summed, value_up, precision=lax.Precision.HIGHEST)

    far_peak, far_total, far_sum = combined_all(
        (block_peak, block_total, to_values(block_sum)), "kv", combine
    )
    near_sum = to_values(own_sum)
    joint_peak, joint_total, joint_sum = combine(
        (far_peak, far_total, far_sum), (own_peak, own_total, near_sum)
    )
    attended = joint_sum / joint_total[..., None]
    values_low = attended.astype(jnp.bfloat16).reshape(row_count, head_count * VDIM)
    projected_part = jnp.dot(values_low, w_out, preferred_element_type=jnp.float32)
    projected = lax.psum(projected_part, "tp")
    squares = lax.psum(jnp.sum(projected * projected, -1), "kv")
    mixed = (projected * lax.rsqrt(squares / D + epsilon)[:, None] * out_gain).astype(jnp.bfloat16)
    return (mixed.reshape(seq_count, prop_count, -1), new_latent, new_rope)


LANES = 128
F32 = jnp.float32
BF16 = jnp.bfloat16
NT = (((1,), (1,)), ((), ()))
TN = (((0,), (1,)), ((), ()))


def lane_of(shape):
    return lax.broadcasted_iota(jnp.int32, shape, len(shape) - 1)


def row_of(shape):
    return lax.broadcasted_iota(jnp.int32, shape, len(shape) - 2)


def fold(top, bottom, low):
    return jnp.where(low, top, pltpu.roll(bottom, 64, 1))


def unfold_pair(first, second, low):
    top = jnp.where(low, first, pltpu.roll(second, 64, 1))
    bottom = jnp.where(low, pltpu.roll(first, 64, 1), second)
    return jnp.concatenate([top, bottom], 0)


def fused_kernel(
    n, seqs, props, shard_len, width,
    parents, lengths, accepted,
    tokens, in_gain, latent_gain, query_gain, key_gain, out_gain, inverse,
    wq_h, wl_h, wr_h, wk_h, wv_h, wo_h, cache_h, rope_h,
    mixed_o, latent_o, rope_o,
    wq, wl, wr, wk, wv, wo, cache, rope,
    x_s, normed_s, keys_s, vhi_s, vlo_s,
    send_a, recv_a, all_a, send_b, recv_b, all_b, proj_s, proj_in, sq_all,
    out_lat, out_rope,
    load_sem, store_sem, ssem, rsem, tsem,
):
    me = lax.axis_index("kv")
    core = lax.axis_index("tp")
    rows = seqs * props
    heads = n
    places = seqs * shard_len

    loads = []
    for at, (src, dst) in enumerate(
        ((wq_h, wq), (wl_h, wl), (cache_h, cache), (rope_h, rope), (wk_h, wk), (wv_h, wv), (wr_h, wr), (wo_h, wo))
    ):
        load = pltpu.make_async_copy(src, dst, load_sem.at[at])
        load.start()
        loads.append(load)

    barrier = pltpu.get_barrier_semaphore()
    for off in range(1, n):
        pl.semaphore_signal(barrier, inc=1, device_id=(lax.rem(me + off, n), core), device_id_type=MESH)
    pl.semaphore_signal(barrier, inc=1, device_id=(me, 1 - core), device_id_type=MESH)

    def copy_to(phase, off, src, dst):
        return pltpu.make_async_remote_copy(
            src_ref=src, dst_ref=dst, send_sem=ssem.at[phase, off], recv_sem=rsem.at[phase, off],
            device_id=(lax.rem(me + off, n), core), device_id_type=MESH,
        )

    def scatter(phase, send, recv):
        for off in range(1, n):
            copy_to(phase, off, send.at[lax.rem(me + off, n)], recv.at[off]).start()

    def scatter_wait(phase, off, send, recv):
        copy_to(phase, off, send.at[lax.rem(me + off, n)], recv.at[off]).wait()

    def gather(phase, table):
        for off in range(1, n):
            copy_to(phase, off, table.at[me], table.at[me]).start()

    def gather_wait(phase, table):
        for off in range(1, n):
            copy_to(phase, off, table.at[me], table.at[lax.rem(me - off + n, n)]).wait_recv()
        for off in range(1, n):
            copy_to(phase, off, table.at[me], table.at[me]).wait_send()

    for s in range(seqs):
        x_s[s * props : (s + 1) * props, :] = tokens[s].astype(F32)
    x = x_s[...]
    normed_s[...] = (x * lax.rsqrt(jnp.mean(x * x, -1, keepdims=True) + epsilon) * in_gain[...]).astype(BF16)
    part_rows = wq.shape[0]
    part = normed_s[:, pl.ds(pl.multiple_of(me * part_rows, part_rows), part_rows)]
    loads[0].wait()
    q_part = jnp.dot(part, wq[...], preferred_element_type=F32)
    loads[1].wait()
    l_part = jnp.dot(part, wl[...], preferred_element_type=F32)
    low8 = lane_of((8, LANES)) < 64
    for h in range(heads):
        if h < heads - 1:
            piece = q_part[:, h * QK : h * QK + LANES]
        else:
            piece = jnp.concatenate([q_part[:, h * QK :], jnp.zeros((rows, LANES - QK), F32)], 1)
        send_a[h, 0:rows, :] = piece
    for m in range(n // 2):
        top = l_part[0:8, m * LANES : (m + 1) * LANES]
        bottom = l_part[8:16, m * LANES : (m + 1) * LANES]
        send_a[2 * m, rows : rows + 8, :] = fold(top, bottom, low8)
        send_a[2 * m + 1, rows : rows + 8, :] = jnp.where(low8, pltpu.roll(top, 64, 1), bottom)
    pl.semaphore_wait(barrier, n)
    scatter(0, send_a, recv_a)

    lane = lane_of((rows, LANES))
    row = row_of((rows, LANES))
    anchors = [lengths[s] + accepted[s] for s in range(seqs)]
    position = jnp.zeros((rows, LANES), jnp.int32)
    seen_own = jnp.zeros((rows, LANES), jnp.int32)
    for s in range(seqs):
        table = []
        for i in range(props):
            line = []
            for j in range(props):
                if j > i:
                    line.append(None)
                elif j == i:
                    line.append(jnp.int32(1))
                else:
                    hit = jnp.int32(0)
                    for m in range(j, i):
                        hit = hit + jnp.where(parents[s, i] == m, table[m][j], 0)
                    line.append(hit)
            table.append(line)
            at = anchors[s] + sum(line[1 : i + 1], line[0]) - 1
            position = jnp.where(row == s * props + i, at, position)
            for j in range(i + 1):
                here = (row == s * props + i) & (lane == s * props + j)
                seen_own = jnp.where(here, line[j], seen_own)
    angle = position.astype(F32) * inverse[...]
    cosine = jnp.cos(angle)
    sine = jnp.where(lane < NOPE + ROPE // 2, -jnp.sin(angle), jnp.sin(angle))

    groups = heads // 4
    pad = jnp.zeros((1, LANES - QK), F32)
    key_gain_row = jnp.concatenate([key_gain[...], pad], 1)
    gain_col = jnp.transpose(jnp.broadcast_to(key_gain_row, (LANES, LANES)))[:, 0:1]
    loads[2].wait()
    loads[3].wait()
    loads[4].wait()
    cached = cache[...].reshape(places, width)
    eye = (row_of((ROPE, ROPE)) == lane_of((ROPE, ROPE))).astype(BF16)
    rope_t = lax.dot_general(eye, rope[...].reshape(places, ROPE), NT, preferred_element_type=F32)
    rope_sq = jnp.sum(rope_t * rope_t, 0, keepdims=True)
    rope_gained = gain_col[NOPE:QK, :]
    for g in range(groups):
        nope_t = lax.dot_general(wk[:, g * 256 : (g + 1) * 256], cached, TN, preferred_element_type=F32)
        for j in range(4):
            nope = nope_t[j * NOPE : (j + 1) * NOPE, :]
            factor = lax.rsqrt((jnp.sum(nope * nope, 0, keepdims=True) + rope_sq) / QK + epsilon)
            keys_s[g, j * NOPE : (j + 1) * NOPE, :] = (nope * factor * gain_col[0:NOPE, :]).astype(BF16)
            keys_s[g, 256 + j * ROPE : 256 + (j + 1) * ROPE, :] = (rope_t * factor * rope_gained).astype(BF16)

    total = send_a[me]
    for off in range(1, n):
        scatter_wait(0, off, send_a, recv_a)
        total = total + recv_a[off]
    q = jnp.where(lane < QK, total[0:rows], 0.0)
    half = ROPE // 2

    def turn(v, cos, sin, split):
        other = jnp.where(lane < split, pltpu.roll(v, LANES - half, 1), pltpu.roll(v, half, 1))
        return v * cos + other * sin

    q = turn(q, cosine, sine, NOPE + half)
    q = jnp.where(lane < QK, q, 0.0)
    query_gain_row = jnp.concatenate([query_gain[...], pad], 1)
    q = q * lax.rsqrt(jnp.sum(q * q, -1, keepdims=True) / QK + epsilon) * query_gain_row
    my_query = q.astype(BF16)
    all_a[me, 0:rows, :] = my_query.astype(F32)
    all_a[me, rows : rows + 8, :] = total[rows : rows + 8]
    gather(1, all_a)

    loads[5].wait()
    for g in range(groups):
        value = jnp.dot(cached, wv[:, g * 256 : (g + 1) * 256], preferred_element_type=F32)
        high = value.astype(BF16)
        vhi_s[:, g * 256 : (g + 1) * 256] = high
        vlo_s[:, g * 256 : (g + 1) * 256] = (value - high.astype(F32)).astype(BF16)
    loads[6].wait()
    rope_raw = jnp.dot(normed_s[...], wr[...], preferred_element_type=F32)
    rope_raw = jnp.concatenate([rope_raw, jnp.zeros((rows, LANES - ROPE), F32)], 1)
    rope_new = turn(rope_raw, pltpu.roll(cosine, 64, 1), pltpu.roll(sine, 64, 1), half)
    rope_new = jnp.where(lane < ROPE, rope_new, 0.0).astype(BF16)

    gather_wait(1, all_a)
    tall = 4 * rows
    row4 = row_of((tall, LANES))
    lane4 = lane_of((tall, LANES))
    seq4 = lax.rem(row4, rows) // props
    anchor4 = jnp.zeros((tall, LANES), jnp.int32)
    for s in range(seqs):
        anchor4 = jnp.where(seq4 == s, anchors[s], anchor4)
    seen = me * shard_len + lane4 < anchor4
    head4 = row4 // rows
    for g in range(groups):
        parts = [all_a[4 * g + j, 0:rows, :] for j in range(4)]
        stacked = jnp.concatenate(parts, 0)
        twice = jnp.where(lane4 < 64, stacked, pltpu.roll(stacked, 64, 1))
        halves = [jnp.where(head4 == 2 * c + lane4 // 64, twice, 0.0) for c in range(2)]
        turned = jnp.concatenate([pltpu.roll(parts[j], (64 + 32 * j) % LANES, 1) if j != 2 else parts[j] for j in range(4)], 0)
        turned = jnp.where(head4 == lane4 // ROPE, turned, 0.0)
        wide_q = jnp.concatenate(halves + [turned], 1).astype(BF16)
        scores = jnp.dot(wide_q, keys_s[g], preferred_element_type=F32)
        mine = scores[:, 0:shard_len]
        for s in range(1, seqs):
            mine = jnp.where(seq4 == s, scores[:, s * shard_len : (s + 1) * shard_len], mine)
        mine = jnp.where(seen, mine * QK ** (-0.5), -1e30)
        peak = jnp.max(mine, -1, keepdims=True)
        weights = jnp.where(seen, jnp.exp(mine - peak), 0.0)
        totals = jnp.sum(weights, -1, keepdims=True)
        spread = jnp.concatenate([jnp.where(seq4 == s, weights, 0.0) for s in range(seqs)], 1).astype(BF16)
        summed = jnp.dot(spread, vhi_s[:, g * 256 : (g + 1) * 256], preferred_element_type=F32)
        summed = summed + jnp.dot(spread, vlo_s[:, g * 256 : (g + 1) * 256], preferred_element_type=F32)
        for j in range(4):
            block = slice(j * rows, (j + 1) * rows)
            here = summed[block, (j // 2) * LANES : (j // 2 + 1) * LANES]
            if j % 2:
                here = pltpu.roll(here, 64, 1)
            send_b[4 * g + j] = jnp.where(lane < 64, here, jnp.where(lane < 96, peak[block], totals[block]))
    scatter(2, send_b, recv_b)

    latent = jnp.concatenate(
        [unfold_pair(all_a[2 * m, rows : rows + 8, :], all_a[2 * m + 1, rows : rows + 8, :], low8) for m in range(n // 2)], 1
    )
    latent_new = (
        latent * lax.rsqrt(jnp.mean(latent * latent, -1, keepdims=True) + epsilon) * latent_gain[...]
    ).astype(BF16)

    pair = pl.ds(pl.multiple_of((me // 2) * LANES, LANES), LANES)
    odd = jnp.broadcast_to(lax.rem(me, 2), (rows, LANES)) == 1

    def of_head(both):
        return jnp.where(odd, pltpu.roll(both, 64, 1), both)

    own_nope = of_head(jnp.dot(latent_new, wk[:, pair], preferred_element_type=F32))
    own_key = jnp.where(lane < NOPE, own_nope, pltpu.roll(rope_new.astype(F32), 64, 1))
    own_key = jnp.where(lane < QK, own_key, 0.0)
    own_key = own_key * lax.rsqrt(jnp.sum(own_key * own_key, -1, keepdims=True) / QK + epsilon) * key_gain_row
    own_scores = lax.dot_general(
        my_query, jnp.concatenate([own_key, jnp.zeros((LANES - rows, LANES), F32)], 0).astype(BF16),
        NT, preferred_element_type=F32,
    )
    own_seen = seen_own > 0
    own_scores = jnp.where(own_seen, own_scores * QK ** (-0.5), -1e30)
    own_peak = jnp.max(own_scores, -1, keepdims=True)
    own_weights = jnp.where(own_seen, jnp.exp(own_scores - own_peak), 0.0)
    own_total = jnp.sum(own_weights, -1, keepdims=True)
    own_value = of_head(jnp.dot(latent_new, wv[:, pair], preferred_element_type=F32))
    own_value = jnp.concatenate([own_value, jnp.zeros((LANES - rows, LANES), F32)], 0)
    own_high = own_value.astype(BF16)
    own_low = (own_value - own_high.astype(F32)).astype(BF16)
    own_low_weights = own_weights.astype(BF16)
    own_sum = jnp.dot(own_low_weights, own_high, preferred_element_type=F32)
    own_sum = own_sum + jnp.dot(own_low_weights, own_low, preferred_element_type=F32)

    slot = lane_of((shard_len, rows))
    stores = []
    for s in range(seqs):
        offset = me * shard_len + row_of((shard_len, rows)) - anchors[s]
        chosen = ((slot // props == s) & (offset == lax.rem(slot, props))).astype(F32).astype(BF16)
        put = jnp.dot(chosen, latent_new, preferred_element_type=F32)
        wide = me * shard_len + row_of((shard_len, width)) - anchors[s]
        filled = (wide >= 0) & (wide < props)
        out_lat[s] = jnp.where(filled, put, cache[s].astype(F32)).astype(BF16)
        put_rope = jnp.dot(chosen, rope_new, preferred_element_type=F32)[:, 0:ROPE]
        thin = me * shard_len + row_of((shard_len, ROPE)) - anchors[s]
        out_rope[s] = jnp.where((thin >= 0) & (thin < props), put_rope, rope[s].astype(F32)).astype(BF16)
    for at, (src, dst) in enumerate(((out_lat, latent_o), (out_rope, rope_o))):
        store = pltpu.make_async_copy(src, dst, store_sem.at[at])
        store.start()
        stores.append(store)

    pieces = [send_b[me]]
    for off in range(1, n):
        scatter_wait(2, off, send_b, recv_b)
        pieces.append(recv_b[off])
    peaks = [piece[:, 64:65] for piece in pieces]
    highest = own_peak
    for peak in peaks:
        highest = jnp.maximum(highest, peak)
    scale = jnp.exp(own_peak - highest)
    joint_sum = own_sum * scale
    joint_total = own_total * scale
    for piece, peak in zip(pieces, peaks):
        scale = jnp.exp(peak - highest)
        joint_sum = joint_sum + piece * scale
        joint_total = joint_total + piece[:, 96:97] * scale
    values_low = (joint_sum / joint_total).astype(BF16).astype(F32)
    all_b[me] = fold(values_low[0:8], values_low[8:16], low8)
    gather(3, all_b)
    loads[7].wait()
    gather_wait(3, all_b)
    values = jnp.concatenate(
        [unfold_pair(all_b[2 * m], all_b[2 * m + 1], low8) for m in range(n // 2)], 1
    ).astype(BF16)

    proj_s[...] = jnp.dot(values, wo[...], preferred_element_type=F32)
    swap = pltpu.make_async_remote_copy(
        src_ref=proj_s, dst_ref=proj_in, send_sem=tsem.at[0], recv_sem=tsem.at[1],
        device_id=(me, 1 - core), device_id_type=MESH,
    )
    swap.start()
    swap.wait()
    projected = proj_s[...] + proj_in[...]
    squares = jnp.broadcast_to(jnp.sum(projected * projected, -1, keepdims=True), (rows, LANES))
    sq_all[me] = jnp.where(low8, squares[0:8], squares[8:16])
    gather(4, sq_all)
    gather_wait(4, sq_all)
    squares = sq_all[0]
    for k in range(1, n):
        squares = squares + sq_all[k]
    squares = jnp.concatenate([squares[:, 0:1], squares[:, 64:65]], 0)
    model_width = x_s.shape[1]
    mixed = (projected * lax.rsqrt(squares / model_width + epsilon) * out_gain[...]).astype(BF16)
    for s in range(seqs):
        mixed_o[s] = mixed[s * props : (s + 1) * props, :]
    for store in stores:
        store.wait()


def fused(
    n, tokens, parents, lengths, accepted, in_gain, w_query, w_latent, w_rope_key, latent_gain, query_gain,
    key_gain, w_key_up, w_value_up, w_out, out_gain, cache_latent, cache_rope,
):
    seqs, props, model_width = tokens.shape
    shard_len, width = cache_latent.shape[1:]
    rows = seqs * props
    places = seqs * shard_len
    heads_wide = w_value_up.shape[1]
    out_cols = w_out.shape[1]
    half = ROPE // 2
    wave = rope_base ** (-np.arange(half, dtype=np.float32) / np.float32(half))
    inverse = np.zeros((1, LANES), np.float32)
    inverse[0, NOPE : NOPE + half] = wave
    inverse[0, NOPE + half : QK] = wave
    smem = pl.BlockSpec(memory_space=pltpu.SMEM)
    vmem = pl.BlockSpec(memory_space=pltpu.VMEM)
    hbm = pl.BlockSpec(memory_space=pl.ANY)
    held = [w_query, w_latent, w_rope_key, w_key_up, w_value_up, w_out, cache_latent, cache_rope]
    return pl.pallas_call(
        functools.partial(fused_kernel, n, seqs, props, shard_len, width),
        out_shape=(
            jax.ShapeDtypeStruct((seqs, props, out_cols), BF16),
            jax.ShapeDtypeStruct(cache_latent.shape, BF16),
            jax.ShapeDtypeStruct(cache_rope.shape, BF16),
        ),
        in_specs=[smem] * 3 + [vmem] * 7 + [hbm] * 8,
        out_specs=(vmem, hbm, hbm),
        scratch_shapes=[pltpu.VMEM(array.shape, array.dtype) for array in held]
        + [
            pltpu.VMEM((rows, model_width), F32),
            pltpu.VMEM((rows, model_width), BF16),
            pltpu.VMEM((n // 4, 4 * QK, places), BF16),
            pltpu.VMEM((places, heads_wide), BF16),
            pltpu.VMEM((places, heads_wide), BF16),
            pltpu.VMEM((n, rows + 8, LANES), F32),
            pltpu.VMEM((n, rows + 8, LANES), F32),
            pltpu.VMEM((n, rows + 8, LANES), F32),
            pltpu.VMEM((n, rows, LANES), F32),
            pltpu.VMEM((n, rows, LANES), F32),
            pltpu.VMEM((n, 8, LANES), F32),
            pltpu.VMEM((rows, out_cols), F32),
            pltpu.VMEM((rows, out_cols), F32),
            pltpu.VMEM((n, 8, LANES), F32),
            pltpu.VMEM(cache_latent.shape, BF16),
            pltpu.VMEM(cache_rope.shape, BF16),
            pltpu.SemaphoreType.DMA((len(held),)),
            pltpu.SemaphoreType.DMA((2,)),
            pltpu.SemaphoreType.DMA((5, n)),
            pltpu.SemaphoreType.DMA((5, n)),
            pltpu.SemaphoreType.DMA((2,)),
        ],
        compiler_params=pltpu.CompilerParams(
            collective_id=0, has_side_effects=True, vmem_limit_bytes=56 * 1024 * 1024
        ),
    )(
        parents, lengths, accepted, tokens, in_gain.reshape(1, -1), latent_gain.reshape(1, -1),
        query_gain.reshape(1, -1), key_gain.reshape(1, -1), out_gain.reshape(1, -1), jnp.asarray(inverse), *held,
    )


def step(n, cores, tokens, *others):
    w_query, w_latent, w_key_up, cache_latent = others[4], others[5], others[10], others[14]
    fits = (
        tokens.shape[0] * tokens.shape[1] == 16
        and cores == 2
        and w_key_up.shape[1] == n * NOPE
        and w_latent.shape[1] == n * 64
        and n % 4 == 0
        and w_query.shape[0] % LANES == 0
        and cache_latent.shape[1] == LANES
    )
    if fits:
        return fused(n, tokens, *others)
    return body(tokens, *others)


def solution(mesh):
    return jax.shard_map(
        functools.partial(step, mesh.shape["kv"], mesh.shape["tp"]),
        mesh=mesh,
        in_specs=(
            P(),
            P(),
            P(),
            P(),
            P(),
            P("kv", "tp"),
            P("kv", None),
            P(),
            P(),
            P(),
            P(),
            P(None, "tp"),
            P(None, "tp"),
            P("tp", "kv"),
            P("kv"),
            P(None, "kv", None),
            P(None, "kv", None),
        ),
        out_specs=(P(None, None, "kv"), P(None, "kv", None), P(None, "kv", None)),
        check_vma=False,
    )
```

```python
import functools

import jax
import jax.numpy as jnp
import numpy as np
from jax import lax
from jax.experimental import pallas as pl
from jax.experimental.pallas import tpu as pltpu
from jax.sharding import PartitionSpec as P

MESH = pl.DeviceIdType.MESH

D = 4096
NOPE = 64
ROPE = 32
QK = 96
VDIM = 64


epsilon = 1e-06
rope_base = 10000.0


def combined_all(value, axis, join):
    pieces = jax.tree.map(lambda part: lax.all_gather(part, axis), value)
    head = jax.tree.map(lambda part: part[0], pieces)
    tail = jax.tree.map(lambda part: part[1:], pieces)
    running, _ = lax.scan(lambda running, piece: (join(running, piece), None), head, tail)
    return running


def ancestry(parents):
    prop_count = parents.shape[-1]
    indices = jnp.arange(prop_count, dtype=jnp.int32)
    step_map = (parents[..., :, None] == indices).astype(jnp.int32)
    identity_map = jnp.broadcast_to(
        (indices[:, None] == indices[None, :]).astype(jnp.int32), step_map.shape
    )
    reached = identity_map
    hop_map = identity_map
    for step_index in range(prop_count - 1):
        hop_map = jnp.einsum("sij,sjk->sik", hop_map, step_map)
        reached = reached + hop_map
    return reached


def angles(positions):
    halfway = ROPE // 2
    inverse = rope_base ** (-jnp.arange(halfway, dtype=jnp.float32) / halfway)
    angle = positions.astype(jnp.float32)[..., None] * inverse
    return (jnp.cos(angle), jnp.sin(angle))


def rotate(vectors, cosine, sine_part):
    halfway = vectors.shape[-1] // 2
    leading = vectors[..., :halfway]
    trailing = vectors[..., halfway:]
    return jnp.concatenate(
        [leading * cosine - trailing * sine_part, trailing * cosine + leading * sine_part], -1
    )


def split_keys(latents, rope_rows, w_key_up, key_gain):
    head_count = w_key_up.shape[1] // NOPE
    nope = jnp.dot(latents, w_key_up, preferred_element_type=jnp.float32)
    nope = nope.reshape(latents.shape[:2] + (head_count, NOPE))
    rope_wide = rope_rows.astype(jnp.float32)[:, :, None, :]
    squares = jnp.sum(nope * nope, -1) + jnp.sum(rope_wide * rope_wide, -1)
    factor = lax.rsqrt(squares / QK + epsilon)[..., None]
    key_nope = (nope * factor * key_gain[:NOPE]).astype(jnp.bfloat16)
    key_rope = (rope_wide * factor * key_gain[NOPE:]).astype(jnp.bfloat16)
    return (key_nope, key_rope)


def attend_block(query, key_nope, key_rope, latents, visible):
    score_scale = QK ** (-0.5)
    scores = jnp.einsum(
        "sphd,slhd->shpl", query[..., :NOPE], key_nope, preferred_element_type=jnp.float32
    )
    scores = scores + jnp.einsum(
        "sphd,slhd->shpl", query[..., NOPE:], key_rope, preferred_element_type=jnp.float32
    )
    scores = jnp.where(visible, scores * score_scale, -1e30)
    peaks = jnp.max(scores, -1)
    weights = jnp.where(visible, jnp.exp(scores - peaks[..., None]), 0.0)
    totals = jnp.sum(weights, -1)
    summed = jnp.einsum(
        "shpl,slc->sphc", weights.astype(jnp.bfloat16), latents, preferred_element_type=jnp.float32
    )
    return (jnp.swapaxes(peaks, 1, 2), jnp.swapaxes(totals, 1, 2), summed)


def combine(left_part, right_part):
    left_peak, left_total, left_sum = left_part
    right_peak, right_total, right_sum = right_part
    highest = jnp.maximum(left_peak, right_peak)
    left_scale = jnp.exp(left_peak - highest)
    right_scale = jnp.exp(right_peak - highest)
    return (
        highest,
        left_total * left_scale + right_total * right_scale,
        left_sum * left_scale[..., None] + right_sum * right_scale[..., None],
    )


def body(
    tokens,
    parents,
    lengths,
    accepted,
    in_gain,
    w_query,
    w_latent,
    w_rope_key,
    latent_gain,
    query_gain,
    key_gain,
    w_key_up,
    w_value_up,
    w_out,
    out_gain,
    cache_latent,
    cache_rope,
):
    seq_count, prop_count, model_width = tokens.shape
    row_count = seq_count * prop_count
    head_count = w_key_up.shape[1] // NOPE
    flattened = tokens.reshape(row_count, model_width).astype(jnp.float32)
    normed = (
        flattened
        * lax.rsqrt(jnp.mean(flattened * flattened, -1, keepdims=True) + epsilon)
        * in_gain
    ).astype(jnp.bfloat16)
    part_rows = w_query.shape[0]
    normed_part = lax.dynamic_slice_in_dim(normed, lax.axis_index("kv") * part_rows, part_rows, 1)
    query_part = jnp.dot(normed_part, w_query, preferred_element_type=jnp.float32)
    latent_part = jnp.dot(normed_part, w_latent, preferred_element_type=jnp.float32)
    query_raw, latent_raw = lax.psum((query_part, latent_part), "kv")
    rope_raw = jnp.dot(normed, w_rope_key, preferred_element_type=jnp.float32).reshape(
        seq_count, prop_count, ROPE
    )
    latent_raw = latent_raw.reshape(seq_count, prop_count, -1)
    reached = ancestry(parents)
    anchor = lengths + accepted
    positions = anchor[:, None] + jnp.sum(reached, -1) - 1
    cosine, sine_part = angles(positions)
    query_raw = query_raw.reshape(seq_count, prop_count, head_count, QK)
    turned = rotate(query_raw[..., NOPE:], cosine[:, :, None, :], sine_part[:, :, None, :])
    joined = jnp.concatenate([query_raw[..., :NOPE], turned], -1)
    query = (
        joined * lax.rsqrt(jnp.mean(joined * joined, -1, keepdims=True) + epsilon) * query_gain
    ).astype(jnp.bfloat16)
    latent_new = (
        latent_raw
        * lax.rsqrt(jnp.mean(latent_raw * latent_raw, -1, keepdims=True) + epsilon)
        * latent_gain
    ).astype(jnp.bfloat16)
    rope_new = rotate(rope_raw, cosine, sine_part).astype(jnp.bfloat16)
    shard_len = cache_latent.shape[1]
    places = lax.axis_index("kv") * shard_len + jnp.arange(shard_len, dtype=jnp.int32)
    offset = places[None, :] - anchor[:, None]
    selected = offset[:, :, None] == jnp.arange(prop_count, dtype=jnp.int32)[None, None, :]
    filled = jnp.any(selected, -1)[..., None]
    selector = selected.astype(jnp.bfloat16)
    placed_latent = jnp.einsum(
        "slp,spc->slc", selector, latent_new, preferred_element_type=jnp.float32
    ).astype(jnp.bfloat16)
    placed_rope = jnp.einsum(
        "slp,spc->slc", selector, rope_new, preferred_element_type=jnp.float32
    ).astype(jnp.bfloat16)
    new_latent = jnp.where(filled, placed_latent, cache_latent)
    new_rope = jnp.where(filled, placed_rope, cache_rope)
    key_nope, key_rope = split_keys(cache_latent, cache_rope, w_key_up, key_gain)
    cache_seen = (places[None, :] < anchor[:, None])[:, None, None, :]
    block_peak, block_total, block_sum = attend_block(
        query, key_nope, key_rope, cache_latent, cache_seen
    )
    own_nope, own_rope = split_keys(latent_new, rope_new, w_key_up, key_gain)
    own_seen = (reached > 0)[:, None, :, :]
    own_peak, own_total, own_sum = attend_block(query, own_nope, own_rope, latent_new, own_seen)
    value_up = w_value_up.astype(jnp.float32).reshape(w_value_up.shape[0], head_count, VDIM)

    def to_values(summed):
        return jnp.einsum("sphc,chd->sphd", summed, value_up, precision=lax.Precision.HIGHEST)

    far_peak, far_total, far_sum = combined_all(
        (block_peak, block_total, to_values(block_sum)), "kv", combine
    )
    near_sum = to_values(own_sum)
    joint_peak, joint_total, joint_sum = combine(
        (far_peak, far_total, far_sum), (own_peak, own_total, near_sum)
    )
    attended = joint_sum / joint_total[..., None]
    values_low = attended.astype(jnp.bfloat16).reshape(row_count, head_count * VDIM)
    projected_part = jnp.dot(values_low, w_out, preferred_element_type=jnp.float32)
    projected = lax.psum(projected_part, "tp")
    squares = lax.psum(jnp.sum(projected * projected, -1), "kv")
    mixed = (projected * lax.rsqrt(squares / D + epsilon)[:, None] * out_gain).astype(jnp.bfloat16)
    return (mixed.reshape(seq_count, prop_count, -1), new_latent, new_rope)


LANES = 128
F32 = jnp.float32
BF16 = jnp.bfloat16
NT = (((1,), (1,)), ((), ()))
TN = (((0,), (1,)), ((), ()))


def lane_of(shape):
    return lax.broadcasted_iota(jnp.int32, shape, len(shape) - 1)


def row_of(shape):
    return lax.broadcasted_iota(jnp.int32, shape, len(shape) - 2)


def fold(top, bottom, low):
    return jnp.where(low, top, pltpu.roll(bottom, 64, 1))


def unfold_pair(first, second, low):
    top = jnp.where(low, first, pltpu.roll(second, 64, 1))
    bottom = jnp.where(low, pltpu.roll(first, 64, 1), second)
    return jnp.concatenate([top, bottom], 0)


def fused_kernel(
    n, seqs, props, shard_len, width,
    parents, lengths, accepted,
    tokens, in_gain, latent_gain, query_gain, key_gain, out_gain, inverse,
    wq_h, wl_h, wr_h, wk_h, wv_h, wo_h, cache_h, rope_h,
    mixed_o, latent_o, rope_o,
    wq, wl, wr, wk, wv, wo, cache, rope,
    x_s, normed_s, keys_s, vhi_s, vlo_s,
    send_a, recv_a, all_a, send_b, recv_b, all_b, proj_s, proj_in, sq_all, lat_s,
    load_sem, ssem, rsem, tsem,
):
    me = lax.axis_index("kv")
    core = lax.axis_index("tp")
    rows = seqs * props
    heads = n
    places = seqs * shard_len

    order = sorted(range(1, n), key=lambda off: abs(off - n // 2))
    loads = []
    for at, (src, dst) in enumerate(
        ((wq_h, wq), (wl_h, wl), (cache_h, cache), (rope_h, rope), (wk_h, wk), (wv_h, wv), (wr_h, wr), (wo_h, wo))
    ):
        load = pltpu.make_async_copy(src, dst, load_sem.at[at])
        load.start()
        loads.append(load)

    barrier = pltpu.get_barrier_semaphore()
    for off in order:
        pl.semaphore_signal(barrier, inc=1, device_id=(lax.rem(me + off, n), core), device_id_type=MESH)
    pl.semaphore_signal(barrier, inc=1, device_id=(me, 1 - core), device_id_type=MESH)

    def copy_to(phase, off, src, dst):
        return pltpu.make_async_remote_copy(
            src_ref=src, dst_ref=dst, send_sem=ssem.at[phase, off], recv_sem=rsem.at[phase, off],
            device_id=(lax.rem(me + off, n), core), device_id_type=MESH,
        )

    def scatter(phase, send, recv):
        for off in order:
            copy_to(phase, off, send.at[lax.rem(me + off, n)], recv.at[off]).start()

    def scatter_wait(phase, off, send, recv):
        copy_to(phase, off, send.at[lax.rem(me + off, n)], recv.at[off]).wait()

    def gather(phase, table):
        for off in order:
            copy_to(phase, off, table.at[me], table.at[me]).start()

    def gather_wait(phase, table):
        for off in order:
            copy_to(phase, off, table.at[me], table.at[lax.rem(me - off + n, n)]).wait_recv()
        for off in order:
            copy_to(phase, off, table.at[me], table.at[me]).wait_send()

    for s in range(seqs):
        x_s[s * props : (s + 1) * props, :] = tokens[s].astype(F32)
    x = x_s[...]
    normed_s[...] = (x * lax.rsqrt(jnp.mean(x * x, -1, keepdims=True) + epsilon) * in_gain[...]).astype(BF16)
    part_rows = wq.shape[0]
    part = normed_s[:, pl.ds(pl.multiple_of(me * part_rows, part_rows), part_rows)]
    loads[0].wait()
    q_part = jnp.dot(part, wq[...], preferred_element_type=F32)
    loads[1].wait()
    l_part = jnp.dot(part, wl[...], preferred_element_type=F32)
    lane = lane_of((rows, LANES))
    row = row_of((rows, LANES))
    low8 = lane_of((8, LANES)) < 64
    first_core = jnp.broadcast_to(core, (8, width)) == 0
    l_half = jnp.where(first_core, l_part[0:8], l_part[8:16])
    for h in range(heads):
        if h < heads - 1:
            piece = q_part[:, h * QK : h * QK + LANES]
        else:
            piece = jnp.concatenate([q_part[:, h * QK :], jnp.zeros((rows, LANES - QK), F32)], 1)
        both = l_half[:, (h // 2) * LANES : (h // 2 + 1) * LANES]
        if h % 2:
            rest = [pltpu.roll(both, 32, 1), both]
        else:
            rest = [pltpu.roll(both, 96, 1), pltpu.roll(both, 64, 1)]
        send_a[h] = jnp.where(lane < QK, piece, jnp.concatenate(rest, 0))
    pl.semaphore_wait(barrier, n)
    scatter(0, send_a, recv_a)

    anchors = [lengths[s] + accepted[s] for s in range(seqs)]
    position = jnp.zeros((rows, LANES), jnp.int32)
    seen_own = jnp.zeros((rows, LANES), jnp.int32)
    for s in range(seqs):
        table = []
        for i in range(props):
            line = []
            for j in range(props):
                if j > i:
                    line.append(None)
                elif j == i:
                    line.append(jnp.int32(1))
                else:
                    hit = jnp.int32(0)
                    for m in range(j, i):
                        hit = hit + jnp.where(parents[s, i] == m, table[m][j], 0)
                    line.append(hit)
            table.append(line)
            at = anchors[s] + sum(line[1 : i + 1], line[0]) - 1
            position = jnp.where(row == s * props + i, at, position)
            for j in range(i + 1):
                here = (row == s * props + i) & (lane == s * props + j)
                seen_own = jnp.where(here, line[j], seen_own)
    angle = position.astype(F32) * inverse[...]
    cosine = jnp.cos(angle)
    sine = jnp.where(lane < NOPE + ROPE // 2, -jnp.sin(angle), jnp.sin(angle))

    groups = heads // 4
    pad = jnp.zeros((1, LANES - QK), F32)
    key_gain_row = jnp.concatenate([key_gain[...], pad], 1)
    gain_col = jnp.transpose(jnp.broadcast_to(key_gain_row, (LANES, LANES)))[:, 0:1]
    loads[2].wait()
    loads[3].wait()
    loads[4].wait()
    cached = cache[...].reshape(places, width)
    rope_t = jnp.concatenate([rope[s].astype(F32) for s in range(seqs)], 1)
    rope_sq = jnp.sum(rope_t * rope_t, 0, keepdims=True)
    rope_gained = gain_col[NOPE:QK, :]
    for g in range(groups):
        nope_t = lax.dot_general(wk[:, g * 256 : (g + 1) * 256], cached, TN, preferred_element_type=F32)
        for j in range(4):
            nope = nope_t[j * NOPE : (j + 1) * NOPE, :]
            factor = lax.rsqrt((jnp.sum(nope * nope, 0, keepdims=True) + rope_sq) / QK + epsilon)
            keys_s[g, j * NOPE : (j + 1) * NOPE, :] = (nope * factor * gain_col[0:NOPE, :]).astype(BF16)
            keys_s[g, 256 + j * ROPE : 256 + (j + 1) * ROPE, :] = (rope_t * factor * rope_gained).astype(BF16)

    total = send_a[me]
    for off in reversed(order):
        scatter_wait(0, off, send_a, recv_a)
        total = total + recv_a[off]
    q = jnp.where(lane < QK, total, 0.0)
    half = ROPE // 2

    def turn(v, cos, sin, split):
        other = jnp.where(lane < split, pltpu.roll(v, LANES - half, 1), pltpu.roll(v, half, 1))
        return v * cos + other * sin

    q = turn(q, cosine, sine, NOPE + half)
    q = jnp.where(lane < QK, q, 0.0)
    query_gain_row = jnp.concatenate([query_gain[...], pad], 1)
    q = q * lax.rsqrt(jnp.sum(q * q, -1, keepdims=True) / QK + epsilon) * query_gain_row
    my_query = q.astype(BF16)
    all_a[me] = jnp.where(lane < QK, my_query.astype(F32), total)
    gather(1, all_a)

    loads[5].wait()
    for g in range(groups):
        value = jnp.dot(cached, wv[:, g * 256 : (g + 1) * 256], preferred_element_type=F32)
        high = value.astype(BF16)
        vhi_s[:, g * 256 : (g + 1) * 256] = high
        vlo_s[:, g * 256 : (g + 1) * 256] = (value - high.astype(F32)).astype(BF16)
    loads[6].wait()
    rope_raw = lax.dot_general(normed_s[...], wr[...], NT, preferred_element_type=F32)
    rope_raw = jnp.concatenate([rope_raw, jnp.zeros((rows, LANES - ROPE), F32)], 1)
    rope_new = turn(rope_raw, pltpu.roll(cosine, 64, 1), pltpu.roll(sine, 64, 1), half)
    rope_new = jnp.where(lane < ROPE, rope_new, 0.0).astype(BF16)

    gather_wait(1, all_a)
    tall = 4 * rows
    row4 = row_of((tall, LANES))
    lane4 = lane_of((tall, LANES))
    seq4 = lax.rem(row4, rows) // props
    anchor4 = jnp.zeros((tall, LANES), jnp.int32)
    for s in range(seqs):
        anchor4 = jnp.where(seq4 == s, anchors[s], anchor4)
    seen = me * shard_len + lane4 < anchor4
    head4 = row4 // rows
    for g in range(groups):
        parts = [all_a[4 * g + j] for j in range(4)]
        stacked = jnp.concatenate(parts, 0)
        twice = jnp.where(lane4 < 64, stacked, pltpu.roll(stacked, 64, 1))
        halves = [jnp.where(head4 == 2 * c + lane4 // 64, twice, 0.0) for c in range(2)]
        turned = jnp.concatenate([pltpu.roll(parts[j], (64 + 32 * j) % LANES, 1) if j != 2 else parts[j] for j in range(4)], 0)
        turned = jnp.where(head4 == lane4 // ROPE, turned, 0.0)
        wide_q = jnp.concatenate(halves + [turned], 1).astype(BF16)
        scores = jnp.dot(wide_q, keys_s[g], preferred_element_type=F32)
        mine = scores[:, 0:shard_len]
        for s in range(1, seqs):
            mine = jnp.where(seq4 == s, scores[:, s * shard_len : (s + 1) * shard_len], mine)
        mine = jnp.where(seen, mine * QK ** (-0.5), -1e30)
        peak = jnp.max(mine, -1, keepdims=True)
        weights = jnp.where(seen, jnp.exp(mine - peak), 0.0)
        totals = jnp.sum(weights, -1, keepdims=True)
        spread = jnp.concatenate([jnp.where(seq4 == s, weights, 0.0) for s in range(seqs)], 1).astype(BF16)
        summed = jnp.dot(spread, vhi_s[:, g * 256 : (g + 1) * 256], preferred_element_type=F32)
        summed = summed + jnp.dot(spread, vlo_s[:, g * 256 : (g + 1) * 256], preferred_element_type=F32)
        for j in range(4):
            block = slice(j * rows, (j + 1) * rows)
            here = summed[block, (j // 2) * LANES : (j // 2 + 1) * LANES]
            if j % 2:
                here = pltpu.roll(here, 64, 1)
            send_b[4 * g + j] = jnp.where(lane < 64, here, jnp.where(lane < 96, peak[block], totals[block]))
    scatter(2, send_b, recv_b)

    lane8 = lane_of((8, LANES))
    blocks = []
    for m in range(n // 2):
        even, odd_part = all_a[2 * m], all_a[2 * m + 1]
        left = jnp.where(lane8 < 32, pltpu.roll(even[0:8], 32, 1), pltpu.roll(even[8:16], 64, 1))
        right = jnp.where(lane8 < 96, pltpu.roll(odd_part[0:8], 96, 1), odd_part[8:16])
        blocks.append(jnp.where(low8, left, right))
    lat_s[core] = jnp.concatenate(blocks, 1)
    pltpu.make_async_remote_copy(
        src_ref=lat_s.at[core], dst_ref=lat_s.at[core], send_sem=tsem.at[2], recv_sem=tsem.at[3],
        device_id=(me, 1 - core), device_id_type=MESH,
    ).start()
    arrived = pltpu.make_async_remote_copy(
        src_ref=lat_s.at[core], dst_ref=lat_s.at[1 - core], send_sem=tsem.at[2], recv_sem=tsem.at[3],
        device_id=(me, 1 - core), device_id_type=MESH,
    )
    arrived.wait()
    latent = jnp.concatenate([lat_s[0], lat_s[1]], 0)
    latent_new = (
        latent * lax.rsqrt(jnp.mean(latent * latent, -1, keepdims=True) + epsilon) * latent_gain[...]
    ).astype(BF16)

    pair = pl.ds(pl.multiple_of((me // 2) * LANES, LANES), LANES)
    odd = jnp.broadcast_to(lax.rem(me, 2), (rows, LANES)) == 1

    def of_head(both):
        return jnp.where(odd, pltpu.roll(both, 64, 1), both)

    own_nope = of_head(jnp.dot(latent_new, wk[:, pair], preferred_element_type=F32))
    own_key = jnp.where(lane < NOPE, own_nope, pltpu.roll(rope_new.astype(F32), 64, 1))
    own_key = jnp.where(lane < QK, own_key, 0.0)
    own_key = own_key * lax.rsqrt(jnp.sum(own_key * own_key, -1, keepdims=True) / QK + epsilon) * key_gain_row
    own_scores = lax.dot_general(
        my_query, jnp.concatenate([own_key, jnp.zeros((LANES - rows, LANES), F32)], 0).astype(BF16),
        NT, preferred_element_type=F32,
    )
    own_seen = seen_own > 0
    own_scores = jnp.where(own_seen, own_scores * QK ** (-0.5), -1e30)
    own_peak = jnp.max(own_scores, -1, keepdims=True)
    own_weights = jnp.where(own_seen, jnp.exp(own_scores - own_peak), 0.0)
    own_total = jnp.sum(own_weights, -1, keepdims=True)
    own_value = of_head(jnp.dot(latent_new, wv[:, pair], preferred_element_type=F32))
    own_value = jnp.concatenate([own_value, jnp.zeros((LANES - rows, LANES), F32)], 0)
    own_high = own_value.astype(BF16)
    own_low = (own_value - own_high.astype(F32)).astype(BF16)
    own_low_weights = own_weights.astype(BF16)
    own_sum = jnp.dot(own_low_weights, own_high, preferred_element_type=F32)
    own_sum = own_sum + jnp.dot(own_low_weights, own_low, preferred_element_type=F32)

    latent_o[...] = latent_new
    rope_o[...] = rope_new

    pieces = [send_b[me]]
    for off in reversed(order):
        scatter_wait(2, off, send_b, recv_b)
        pieces.append(recv_b[off])
    peaks = [piece[:, 64:65] for piece in pieces]
    highest = own_peak
    for peak in peaks:
        highest = jnp.maximum(highest, peak)
    scale = jnp.exp(own_peak - highest)
    joint_sum = own_sum * scale
    joint_total = own_total * scale
    for piece, peak in zip(pieces, peaks):
        scale = jnp.exp(peak - highest)
        joint_sum = joint_sum + piece * scale
        joint_total = joint_total + piece[:, 96:97] * scale
    values_low = (joint_sum / joint_total).astype(BF16).astype(F32)
    all_b[me] = fold(values_low[0:8], values_low[8:16], low8)
    gather(3, all_b)
    loads[7].wait()
    gather_wait(3, all_b)
    values = jnp.concatenate(
        [unfold_pair(all_b[2 * m], all_b[2 * m + 1], low8) for m in range(n // 2)], 1
    ).astype(BF16)

    proj_s[...] = jnp.dot(values, wo[...], preferred_element_type=F32)
    swap = pltpu.make_async_remote_copy(
        src_ref=proj_s, dst_ref=proj_in, send_sem=tsem.at[0], recv_sem=tsem.at[1],
        device_id=(me, 1 - core), device_id_type=MESH,
    )
    swap.start()
    swap.wait()
    projected = proj_s[...] + proj_in[...]
    squares = jnp.sum(projected * projected, -1, keepdims=True)
    on_diagonal = row == lane
    sq_all[me] = jnp.sum(jnp.where(on_diagonal, squares, 0.0), 0, keepdims=True)
    gather(4, sq_all)
    gather_wait(4, sq_all)
    squares = sq_all[0]
    for k in range(1, n):
        squares = squares + sq_all[k]
    squares = jnp.sum(jnp.where(on_diagonal, squares, 0.0), -1, keepdims=True)
    model_width = x_s.shape[1]
    mixed = (projected * lax.rsqrt(squares / model_width + epsilon) * out_gain[...]).astype(BF16)
    for s in range(seqs):
        mixed_o[s] = mixed[s * props : (s + 1) * props, :]


def finish_kernel(
    seqs, props, shard_len, width,
    lengths, accepted, mixed, latent_new, rope_new, rope_in, cache_h,
    mixed_o, rope_o, latent_o, cache, out_lat, load_sem, store_sem,
):
    me = lax.axis_index("kv")
    rows = seqs * props
    loads = [pltpu.make_async_copy(cache_h.at[s], cache.at[s], load_sem.at[s]) for s in range(seqs)]
    for load in loads:
        load.start()
    mixed_o[...] = mixed[...]
    slot = lane_of((shard_len, rows))
    chosen = []
    for s in range(seqs):
        start = lengths[s] + accepted[s] - me * shard_len
        offset = row_of((shard_len, rows)) - start
        chosen.append(((slot // props == s) & (offset == lax.rem(slot, props))).astype(F32).astype(BF16))
        put_rope = lax.dot_general(rope_new[...], chosen[s], TN, preferred_element_type=F32)[0:ROPE]
        across = lane_of((ROPE, shard_len)) - start
        rope_o[s] = jnp.where((across >= 0) & (across < props), put_rope, rope_in[s].astype(F32)).astype(BF16)
    stores = []
    for s in range(seqs):
        put = jnp.dot(chosen[s], latent_new[...], preferred_element_type=F32)
        down = row_of((shard_len, width)) - (lengths[s] + accepted[s] - me * shard_len)
        loads[s].wait()
        out_lat[s] = jnp.where((down >= 0) & (down < props), put, cache[s].astype(F32)).astype(BF16)
        store = pltpu.make_async_copy(out_lat.at[s], latent_o.at[s], store_sem.at[s])
        store.start()
        stores.append(store)
    for store in stores:
        store.wait()


def fused(
    n, tokens, parents, lengths, accepted, in_gain, w_query, w_latent, w_rope_key, latent_gain, query_gain,
    key_gain, w_key_up, w_value_up, w_out, out_gain, cache_latent, cache_rope,
):
    seqs, props, model_width = tokens.shape
    shard_len, width = cache_latent.shape[1:]
    rows = seqs * props
    places = seqs * shard_len
    heads_wide = w_value_up.shape[1]
    out_cols = w_out.shape[1]
    half = ROPE // 2
    wave = rope_base ** (-np.arange(half, dtype=np.float32) / np.float32(half))
    inverse = np.zeros((1, LANES), np.float32)
    inverse[0, NOPE : NOPE + half] = wave
    inverse[0, NOPE + half : QK] = wave
    smem = pl.BlockSpec(memory_space=pltpu.SMEM)
    vmem = pl.BlockSpec(memory_space=pltpu.VMEM)
    hbm = pl.BlockSpec(memory_space=pl.ANY)
    rope_in = jnp.swapaxes(cache_rope, 1, 2)
    held = [w_query, w_latent, w_rope_key.T, w_key_up, w_value_up, w_out, cache_latent, rope_in]
    mixed, latent_new, rope_new = pl.pallas_call(
        functools.partial(fused_kernel, n, seqs, props, shard_len, width),
        out_shape=(
            jax.ShapeDtypeStruct((seqs, props, out_cols), BF16),
            jax.ShapeDtypeStruct((rows, width), BF16),
            jax.ShapeDtypeStruct((rows, LANES), BF16),
        ),
        in_specs=[smem] * 3 + [vmem] * 7 + [hbm] * 8,
        out_specs=(vmem, vmem, vmem),
        scratch_shapes=[pltpu.VMEM(array.shape, array.dtype) for array in held]
        + [
            pltpu.VMEM((rows, model_width), F32),
            pltpu.VMEM((rows, model_width), BF16),
            pltpu.VMEM((n // 4, 4 * QK, places), BF16),
            pltpu.VMEM((places, heads_wide), BF16),
            pltpu.VMEM((places, heads_wide), BF16),
            pltpu.VMEM((n, rows, LANES), F32),
            pltpu.VMEM((n, rows, LANES), F32),
            pltpu.VMEM((n, rows, LANES), F32),
            pltpu.VMEM((n, rows, LANES), F32),
            pltpu.VMEM((n, rows, LANES), F32),
            pltpu.VMEM((n, 8, LANES), F32),
            pltpu.VMEM((rows, out_cols), F32),
            pltpu.VMEM((rows, out_cols), F32),
            pltpu.VMEM((n, 1, LANES), F32),
            pltpu.VMEM((2, rows // 2, width), F32),
            pltpu.SemaphoreType.DMA((len(held),)),
            pltpu.SemaphoreType.DMA((5, n)),
            pltpu.SemaphoreType.DMA((5, n)),
            pltpu.SemaphoreType.DMA((4,)),
        ],
        compiler_params=pltpu.CompilerParams(
            collective_id=0, has_side_effects=True, vmem_limit_bytes=56 * 1024 * 1024
        ),
    )(
        parents, lengths, accepted, tokens, in_gain.reshape(1, -1), latent_gain.reshape(1, -1),
        query_gain.reshape(1, -1), key_gain.reshape(1, -1), out_gain.reshape(1, -1), jnp.asarray(inverse), *held,
    )
    mixed, new_rope, new_latent = pl.pallas_call(
        functools.partial(finish_kernel, seqs, props, shard_len, width),
        out_shape=(
            jax.ShapeDtypeStruct(mixed.shape, BF16),
            jax.ShapeDtypeStruct(rope_in.shape, BF16),
            jax.ShapeDtypeStruct(cache_latent.shape, BF16),
        ),
        in_specs=[smem] * 2 + [vmem] * 4 + [hbm],
        out_specs=(vmem, vmem, hbm),
        scratch_shapes=[
            pltpu.VMEM(cache_latent.shape, BF16),
            pltpu.VMEM(cache_latent.shape, BF16),
            pltpu.SemaphoreType.DMA((seqs,)),
            pltpu.SemaphoreType.DMA((seqs,)),
        ],
    )(lengths, accepted, mixed, latent_new, rope_new, rope_in, cache_latent)
    return mixed, new_latent, jnp.swapaxes(new_rope, 1, 2)


def step(n, cores, tokens, *others):
    w_query, w_latent, w_key_up, cache_latent = others[4], others[5], others[10], others[14]
    fits = (
        tokens.shape[0] * tokens.shape[1] == 16
        and cores == 2
        and w_key_up.shape[1] == n * NOPE
        and w_latent.shape[1] == n * 64
        and n % 4 == 0
        and w_query.shape[0] % LANES == 0
        and cache_latent.shape[1] == LANES
    )
    if fits:
        return fused(n, tokens, *others)
    return body(tokens, *others)


def solution(mesh):
    return jax.shard_map(
        functools.partial(step, mesh.shape["kv"], mesh.shape["tp"]),
        mesh=mesh,
        in_specs=(
            P(),
            P(),
            P(),
            P(),
            P(),
            P("kv", "tp"),
            P("kv", None),
            P(),
            P(),
            P(),
            P(),
            P(None, "tp"),
            P(None, "tp"),
            P("tp", "kv"),
            P("kv"),
            P(None, "kv", None),
            P(None, "kv", None),
        ),
        out_specs=(P(None, None, "kv"), P(None, "kv", None), P(None, "kv", None)),
        check_vma=False,
    )
```

```python
import functools

import jax
import jax.numpy as jnp
import numpy as np
from jax import lax
from jax.experimental import pallas as pl
from jax.experimental.pallas import tpu as pltpu
from jax.sharding import PartitionSpec as P

MESH = pl.DeviceIdType.MESH

D = 4096
NOPE = 64
ROPE = 32
QK = 96
VDIM = 64


epsilon = 1e-06
rope_base = 10000.0


def combined_all(value, axis, join):
    pieces = jax.tree.map(lambda part: lax.all_gather(part, axis), value)
    head = jax.tree.map(lambda part: part[0], pieces)
    tail = jax.tree.map(lambda part: part[1:], pieces)
    running, _ = lax.scan(lambda running, piece: (join(running, piece), None), head, tail)
    return running


def ancestry(parents):
    prop_count = parents.shape[-1]
    indices = jnp.arange(prop_count, dtype=jnp.int32)
    step_map = (parents[..., :, None] == indices).astype(jnp.int32)
    identity_map = jnp.broadcast_to(
        (indices[:, None] == indices[None, :]).astype(jnp.int32), step_map.shape
    )
    reached = identity_map
    hop_map = identity_map
    for step_index in range(prop_count - 1):
        hop_map = jnp.einsum("sij,sjk->sik", hop_map, step_map)
        reached = reached + hop_map
    return reached


def angles(positions):
    halfway = ROPE // 2
    inverse = rope_base ** (-jnp.arange(halfway, dtype=jnp.float32) / halfway)
    angle = positions.astype(jnp.float32)[..., None] * inverse
    return (jnp.cos(angle), jnp.sin(angle))


def rotate(vectors, cosine, sine_part):
    halfway = vectors.shape[-1] // 2
    leading = vectors[..., :halfway]
    trailing = vectors[..., halfway:]
    return jnp.concatenate(
        [leading * cosine - trailing * sine_part, trailing * cosine + leading * sine_part], -1
    )


def split_keys(latents, rope_rows, w_key_up, key_gain):
    head_count = w_key_up.shape[1] // NOPE
    nope = jnp.dot(latents, w_key_up, preferred_element_type=jnp.float32)
    nope = nope.reshape(latents.shape[:2] + (head_count, NOPE))
    rope_wide = rope_rows.astype(jnp.float32)[:, :, None, :]
    squares = jnp.sum(nope * nope, -1) + jnp.sum(rope_wide * rope_wide, -1)
    factor = lax.rsqrt(squares / QK + epsilon)[..., None]
    key_nope = (nope * factor * key_gain[:NOPE]).astype(jnp.bfloat16)
    key_rope = (rope_wide * factor * key_gain[NOPE:]).astype(jnp.bfloat16)
    return (key_nope, key_rope)


def attend_block(query, key_nope, key_rope, latents, visible):
    score_scale = QK ** (-0.5)
    scores = jnp.einsum(
        "sphd,slhd->shpl", query[..., :NOPE], key_nope, preferred_element_type=jnp.float32
    )
    scores = scores + jnp.einsum(
        "sphd,slhd->shpl", query[..., NOPE:], key_rope, preferred_element_type=jnp.float32
    )
    scores = jnp.where(visible, scores * score_scale, -1e30)
    peaks = jnp.max(scores, -1)
    weights = jnp.where(visible, jnp.exp(scores - peaks[..., None]), 0.0)
    totals = jnp.sum(weights, -1)
    summed = jnp.einsum(
        "shpl,slc->sphc", weights.astype(jnp.bfloat16), latents, preferred_element_type=jnp.float32
    )
    return (jnp.swapaxes(peaks, 1, 2), jnp.swapaxes(totals, 1, 2), summed)


def combine(left_part, right_part):
    left_peak, left_total, left_sum = left_part
    right_peak, right_total, right_sum = right_part
    highest = jnp.maximum(left_peak, right_peak)
    left_scale = jnp.exp(left_peak - highest)
    right_scale = jnp.exp(right_peak - highest)
    return (
        highest,
        left_total * left_scale + right_total * right_scale,
        left_sum * left_scale[..., None] + right_sum * right_scale[..., None],
    )


def body(
    tokens,
    parents,
    lengths,
    accepted,
    in_gain,
    w_query,
    w_latent,
    w_rope_key,
    latent_gain,
    query_gain,
    key_gain,
    w_key_up,
    w_value_up,
    w_out,
    out_gain,
    cache_latent,
    cache_rope,
):
    seq_count, prop_count, model_width = tokens.shape
    row_count = seq_count * prop_count
    head_count = w_key_up.shape[1] // NOPE
    flattened = tokens.reshape(row_count, model_width).astype(jnp.float32)
    normed = (
        flattened
        * lax.rsqrt(jnp.mean(flattened * flattened, -1, keepdims=True) + epsilon)
        * in_gain
    ).astype(jnp.bfloat16)
    part_rows = w_query.shape[0]
    normed_part = lax.dynamic_slice_in_dim(normed, lax.axis_index("kv") * part_rows, part_rows, 1)
    query_part = jnp.dot(normed_part, w_query, preferred_element_type=jnp.float32)
    latent_part = jnp.dot(normed_part, w_latent, preferred_element_type=jnp.float32)
    query_raw, latent_raw = lax.psum((query_part, latent_part), "kv")
    rope_raw = jnp.dot(normed, w_rope_key, preferred_element_type=jnp.float32).reshape(
        seq_count, prop_count, ROPE
    )
    latent_raw = latent_raw.reshape(seq_count, prop_count, -1)
    reached = ancestry(parents)
    anchor = lengths + accepted
    positions = anchor[:, None] + jnp.sum(reached, -1) - 1
    cosine, sine_part = angles(positions)
    query_raw = query_raw.reshape(seq_count, prop_count, head_count, QK)
    turned = rotate(query_raw[..., NOPE:], cosine[:, :, None, :], sine_part[:, :, None, :])
    joined = jnp.concatenate([query_raw[..., :NOPE], turned], -1)
    query = (
        joined * lax.rsqrt(jnp.mean(joined * joined, -1, keepdims=True) + epsilon) * query_gain
    ).astype(jnp.bfloat16)
    latent_new = (
        latent_raw
        * lax.rsqrt(jnp.mean(latent_raw * latent_raw, -1, keepdims=True) + epsilon)
        * latent_gain
    ).astype(jnp.bfloat16)
    rope_new = rotate(rope_raw, cosine, sine_part).astype(jnp.bfloat16)
    shard_len = cache_latent.shape[1]
    places = lax.axis_index("kv") * shard_len + jnp.arange(shard_len, dtype=jnp.int32)
    offset = places[None, :] - anchor[:, None]
    selected = offset[:, :, None] == jnp.arange(prop_count, dtype=jnp.int32)[None, None, :]
    filled = jnp.any(selected, -1)[..., None]
    selector = selected.astype(jnp.bfloat16)
    placed_latent = jnp.einsum(
        "slp,spc->slc", selector, latent_new, preferred_element_type=jnp.float32
    ).astype(jnp.bfloat16)
    placed_rope = jnp.einsum(
        "slp,spc->slc", selector, rope_new, preferred_element_type=jnp.float32
    ).astype(jnp.bfloat16)
    new_latent = jnp.where(filled, placed_latent, cache_latent)
    new_rope = jnp.where(filled, placed_rope, cache_rope)
    key_nope, key_rope = split_keys(cache_latent, cache_rope, w_key_up, key_gain)
    cache_seen = (places[None, :] < anchor[:, None])[:, None, None, :]
    block_peak, block_total, block_sum = attend_block(
        query, key_nope, key_rope, cache_latent, cache_seen
    )
    own_nope, own_rope = split_keys(latent_new, rope_new, w_key_up, key_gain)
    own_seen = (reached > 0)[:, None, :, :]
    own_peak, own_total, own_sum = attend_block(query, own_nope, own_rope, latent_new, own_seen)
    value_up = w_value_up.astype(jnp.float32).reshape(w_value_up.shape[0], head_count, VDIM)

    def to_values(summed):
        return jnp.einsum("sphc,chd->sphd", summed, value_up, precision=lax.Precision.HIGHEST)

    far_peak, far_total, far_sum = combined_all(
        (block_peak, block_total, to_values(block_sum)), "kv", combine
    )
    near_sum = to_values(own_sum)
    joint_peak, joint_total, joint_sum = combine(
        (far_peak, far_total, far_sum), (own_peak, own_total, near_sum)
    )
    attended = joint_sum / joint_total[..., None]
    values_low = attended.astype(jnp.bfloat16).reshape(row_count, head_count * VDIM)
    projected_part = jnp.dot(values_low, w_out, preferred_element_type=jnp.float32)
    projected = lax.psum(projected_part, "tp")
    squares = lax.psum(jnp.sum(projected * projected, -1), "kv")
    mixed = (projected * lax.rsqrt(squares / D + epsilon)[:, None] * out_gain).astype(jnp.bfloat16)
    return (mixed.reshape(seq_count, prop_count, -1), new_latent, new_rope)


LANES = 128
F32 = jnp.float32
BF16 = jnp.bfloat16
NT = (((1,), (1,)), ((), ()))
TN = (((0,), (1,)), ((), ()))


def lane_of(shape):
    return lax.broadcasted_iota(jnp.int32, shape, len(shape) - 1)


def row_of(shape):
    return lax.broadcasted_iota(jnp.int32, shape, len(shape) - 2)


def fold(top, bottom, low):
    return jnp.where(low, top, pltpu.roll(bottom, 64, 1))


def unfold_pair(first, second, low):
    top = jnp.where(low, first, pltpu.roll(second, 64, 1))
    bottom = jnp.where(low, pltpu.roll(first, 64, 1), second)
    return jnp.concatenate([top, bottom], 0)


def fused_kernel(
    n, seqs, props, shard_len, width,
    parents, lengths, accepted,
    tokens, in_gain, latent_gain, query_gain, key_gain, out_gain, inverse,
    wq_h, wl_h, wr_h, wk_h, wv_h, wo_h, cache_h, rope_h,
    mixed_o, latent_o, rope_o,
    wq, wl, wr, wk, wv, wo, cache, rope,
    x_s, normed_s, keys_s, vhi_s, vlo_s,
    send_a, recv_a, all_a, send_b, recv_b, all_b, proj_s, proj_in, sq_all, lat_s,
    load_sem, ssem, rsem, tsem,
):
    me = lax.axis_index("kv")
    core = lax.axis_index("tp")
    rows = seqs * props
    heads = n
    places = seqs * shard_len

    order = sorted(range(1, n), key=lambda off: abs(off - n // 2))
    loads = []
    for at, (src, dst) in enumerate(
        ((wq_h, wq), (wl_h, wl), (cache_h, cache), (rope_h, rope), (wk_h, wk), (wv_h, wv), (wr_h, wr), (wo_h, wo))
    ):
        load = pltpu.make_async_copy(src, dst, load_sem.at[at])
        loads.append(load)
    for load in loads[:2]:
        load.start()

    barrier = pltpu.get_barrier_semaphore()
    for off in order:
        pl.semaphore_signal(barrier, inc=1, device_id=(lax.rem(me + off, n), core), device_id_type=MESH)
    pl.semaphore_signal(barrier, inc=1, device_id=(me, 1 - core), device_id_type=MESH)

    def copy_to(phase, off, src, dst):
        return pltpu.make_async_remote_copy(
            src_ref=src, dst_ref=dst, send_sem=ssem.at[phase, off], recv_sem=rsem.at[phase, off],
            device_id=(lax.rem(me + off, n), core), device_id_type=MESH,
        )

    def scatter(phase, send, recv):
        for off in order:
            copy_to(phase, off, send.at[lax.rem(me + off, n)], recv.at[off]).start()

    def scatter_wait(phase, off, send, recv):
        copy_to(phase, off, send.at[lax.rem(me + off, n)], recv.at[off]).wait_recv()

    def gather(phase, table):
        for off in order:
            copy_to(phase, off, table.at[me], table.at[me]).start()

    def gather_wait(phase, table):
        for off in order:
            copy_to(phase, off, table.at[me], table.at[lax.rem(me - off + n, n)]).wait_recv()

    for s in range(seqs):
        x_s[s * props : (s + 1) * props, :] = tokens[s].astype(F32)
    x = x_s[...]
    normed_s[...] = (x * lax.rsqrt(jnp.mean(x * x, -1, keepdims=True) + epsilon) * in_gain[...]).astype(BF16)
    part_rows = wq.shape[0]
    part = normed_s[:, pl.ds(pl.multiple_of(me * part_rows, part_rows), part_rows)]
    loads[0].wait()
    q_part = jnp.dot(part, wq[...], preferred_element_type=F32)
    loads[1].wait()
    for load in loads[2:]:
        load.start()
    l_part = jnp.dot(part, wl[...], preferred_element_type=F32)
    lane = lane_of((rows, LANES))
    row = row_of((rows, LANES))
    low8 = lane_of((8, LANES)) < 64
    first_core = jnp.broadcast_to(core, (8, width)) == 0
    l_half = jnp.where(first_core, l_part[0:8], l_part[8:16])
    for h in range(heads):
        if h < heads - 1:
            piece = q_part[:, h * QK : h * QK + LANES]
        else:
            piece = jnp.concatenate([q_part[:, h * QK :], jnp.zeros((rows, LANES - QK), F32)], 1)
        both = l_half[:, (h // 2) * LANES : (h // 2 + 1) * LANES]
        if h % 2:
            rest = [pltpu.roll(both, 32, 1), both]
        else:
            rest = [pltpu.roll(both, 96, 1), pltpu.roll(both, 64, 1)]
        send_a[h] = jnp.where(lane < QK, piece, jnp.concatenate(rest, 0))
    pl.semaphore_wait(barrier, n)
    scatter(0, send_a, recv_a)

    anchors = [lengths[s] + accepted[s] for s in range(seqs)]
    position = jnp.zeros((rows, LANES), jnp.int32)
    seen_own = jnp.zeros((rows, LANES), jnp.int32)
    for s in range(seqs):
        table = []
        for i in range(props):
            line = []
            for j in range(props):
                if j > i:
                    line.append(None)
                elif j == i:
                    line.append(jnp.int32(1))
                else:
                    hit = jnp.int32(0)
                    for m in range(j, i):
                        hit = hit + jnp.where(parents[s, i] == m, table[m][j], 0)
                    line.append(hit)
            table.append(line)
            at = anchors[s] + sum(line[1 : i + 1], line[0]) - 1
            position = jnp.where(row == s * props + i, at, position)
            for j in range(i + 1):
                here = (row == s * props + i) & (lane == s * props + j)
                seen_own = jnp.where(here, line[j], seen_own)
    angle = position.astype(F32) * inverse[...]
    cosine = jnp.cos(angle)
    sine = jnp.where(lane < NOPE + ROPE // 2, -jnp.sin(angle), jnp.sin(angle))

    groups = heads // 4
    pad = jnp.zeros((1, LANES - QK), F32)
    key_gain_row = jnp.concatenate([key_gain[...], pad], 1)
    gain_col = jnp.transpose(jnp.broadcast_to(key_gain_row, (LANES, LANES)))[:, 0:1]
    loads[2].wait()
    loads[3].wait()
    loads[4].wait()
    cached = cache[...].reshape(places, width)
    rope_t = jnp.concatenate([rope[s].astype(F32) for s in range(seqs)], 1)
    rope_sq = jnp.sum(rope_t * rope_t, 0, keepdims=True)
    rope_gained = gain_col[NOPE:QK, :]
    for g in range(groups):
        nope_t = lax.dot_general(wk[:, g * 256 : (g + 1) * 256], cached, TN, preferred_element_type=F32)
        for j in range(4):
            nope = nope_t[j * NOPE : (j + 1) * NOPE, :]
            factor = lax.rsqrt((jnp.sum(nope * nope, 0, keepdims=True) + rope_sq) / QK + epsilon)
            keys_s[g, j * NOPE : (j + 1) * NOPE, :] = (nope * factor * gain_col[0:NOPE, :]).astype(BF16)
            keys_s[g, 256 + j * ROPE : 256 + (j + 1) * ROPE, :] = (rope_t * factor * rope_gained).astype(BF16)

    total = send_a[me]
    for off in reversed(order):
        scatter_wait(0, off, send_a, recv_a)
        total = total + recv_a[off]
    q = jnp.where(lane < QK, total, 0.0)
    half = ROPE // 2

    def turn(v, cos, sin, split):
        other = jnp.where(lane < split, pltpu.roll(v, LANES - half, 1), pltpu.roll(v, half, 1))
        return v * cos + other * sin

    q = turn(q, cosine, sine, NOPE + half)
    q = jnp.where(lane < QK, q, 0.0)
    query_gain_row = jnp.concatenate([query_gain[...], pad], 1)
    q = q * lax.rsqrt(jnp.sum(q * q, -1, keepdims=True) / QK + epsilon) * query_gain_row
    my_query = q.astype(BF16)
    all_a[me] = jnp.where(lane < QK, my_query.astype(F32), total)
    gather(1, all_a)

    loads[5].wait()
    for g in range(groups):
        value = jnp.dot(cached, wv[:, g * 256 : (g + 1) * 256], preferred_element_type=F32)
        high = value.astype(BF16)
        vhi_s[:, g * 256 : (g + 1) * 256] = high
        vlo_s[:, g * 256 : (g + 1) * 256] = (value - high.astype(F32)).astype(BF16)
    loads[6].wait()
    rope_raw = lax.dot_general(normed_s[...], wr[...], NT, preferred_element_type=F32)
    rope_raw = jnp.concatenate([rope_raw, jnp.zeros((rows, LANES - ROPE), F32)], 1)
    rope_new = turn(rope_raw, pltpu.roll(cosine, 64, 1), pltpu.roll(sine, 64, 1), half)
    rope_new = jnp.where(lane < ROPE, rope_new, 0.0).astype(BF16)

    gather_wait(1, all_a)
    tall = 4 * rows
    row4 = row_of((tall, LANES))
    lane4 = lane_of((tall, LANES))
    seq4 = lax.rem(row4, rows) // props
    anchor4 = jnp.zeros((tall, LANES), jnp.int32)
    for s in range(seqs):
        anchor4 = jnp.where(seq4 == s, anchors[s], anchor4)
    seen = me * shard_len + lane4 < anchor4
    head4 = row4 // rows
    for g in range(groups):
        parts = [all_a[4 * g + j] for j in range(4)]
        stacked = jnp.concatenate(parts, 0)
        twice = jnp.where(lane4 < 64, stacked, pltpu.roll(stacked, 64, 1))
        halves = [jnp.where(head4 == 2 * c + lane4 // 64, twice, 0.0) for c in range(2)]
        turned = jnp.concatenate([pltpu.roll(parts[j], (64 + 32 * j) % LANES, 1) if j != 2 else parts[j] for j in range(4)], 0)
        turned = jnp.where(head4 == lane4 // ROPE, turned, 0.0)
        wide_q = jnp.concatenate(halves + [turned], 1).astype(BF16)
        scores = jnp.dot(wide_q, keys_s[g], preferred_element_type=F32)
        mine = scores[:, 0:shard_len]
        for s in range(1, seqs):
            mine = jnp.where(seq4 == s, scores[:, s * shard_len : (s + 1) * shard_len], mine)
        mine = jnp.where(seen, mine * QK ** (-0.5), -1e30)
        peak = jnp.max(mine, -1, keepdims=True)
        weights = jnp.where(seen, jnp.exp(mine - peak), 0.0)
        totals = jnp.sum(weights, -1, keepdims=True)
        spread = jnp.concatenate([jnp.where(seq4 == s, weights, 0.0) for s in range(seqs)], 1).astype(BF16)
        summed = jnp.dot(spread, vhi_s[:, g * 256 : (g + 1) * 256], preferred_element_type=F32)
        summed = summed + jnp.dot(spread, vlo_s[:, g * 256 : (g + 1) * 256], preferred_element_type=F32)
        for j in range(4):
            block = slice(j * rows, (j + 1) * rows)
            here = summed[block, (j // 2) * LANES : (j // 2 + 1) * LANES]
            if j % 2:
                here = pltpu.roll(here, 64, 1)
            send_b[4 * g + j] = jnp.where(lane < 64, here, jnp.where(lane < 96, peak[block], totals[block]))
    scatter(2, send_b, recv_b)

    lane8 = lane_of((8, LANES))
    blocks = []
    for m in range(n // 2):
        even, odd_part = all_a[2 * m], all_a[2 * m + 1]
        left = jnp.where(lane8 < 32, pltpu.roll(even[0:8], 32, 1), pltpu.roll(even[8:16], 64, 1))
        right = jnp.where(lane8 < 96, pltpu.roll(odd_part[0:8], 96, 1), odd_part[8:16])
        blocks.append(jnp.where(low8, left, right))
    lat_s[core] = jnp.concatenate(blocks, 1)
    pltpu.make_async_remote_copy(
        src_ref=lat_s.at[core], dst_ref=lat_s.at[core], send_sem=tsem.at[2], recv_sem=tsem.at[3],
        device_id=(me, 1 - core), device_id_type=MESH,
    ).start()
    arrived = pltpu.make_async_remote_copy(
        src_ref=lat_s.at[core], dst_ref=lat_s.at[1 - core], send_sem=tsem.at[2], recv_sem=tsem.at[3],
        device_id=(me, 1 - core), device_id_type=MESH,
    )
    arrived.wait()
    latent = jnp.concatenate([lat_s[0], lat_s[1]], 0)
    latent_new = (
        latent * lax.rsqrt(jnp.mean(latent * latent, -1, keepdims=True) + epsilon) * latent_gain[...]
    ).astype(BF16)

    pair = pl.ds(pl.multiple_of((me // 2) * LANES, LANES), LANES)
    odd = jnp.broadcast_to(lax.rem(me, 2), (rows, LANES)) == 1

    def of_head(both):
        return jnp.where(odd, pltpu.roll(both, 64, 1), both)

    own_nope = of_head(jnp.dot(latent_new, wk[:, pair], preferred_element_type=F32))
    own_key = jnp.where(lane < NOPE, own_nope, pltpu.roll(rope_new.astype(F32), 64, 1))
    own_key = jnp.where(lane < QK, own_key, 0.0)
    own_key = own_key * lax.rsqrt(jnp.sum(own_key * own_key, -1, keepdims=True) / QK + epsilon) * key_gain_row
    own_scores = lax.dot_general(
        my_query, jnp.concatenate([own_key, jnp.zeros((LANES - rows, LANES), F32)], 0).astype(BF16),
        NT, preferred_element_type=F32,
    )
    own_seen = seen_own > 0
    own_scores = jnp.where(own_seen, own_scores * QK ** (-0.5), -1e30)
    own_peak = jnp.max(own_scores, -1, keepdims=True)
    own_weights = jnp.where(own_seen, jnp.exp(own_scores - own_peak), 0.0)
    own_total = jnp.sum(own_weights, -1, keepdims=True)
    own_value = of_head(jnp.dot(latent_new, wv[:, pair], preferred_element_type=F32))
    own_value = jnp.concatenate([own_value, jnp.zeros((LANES - rows, LANES), F32)], 0)
    own_high = own_value.astype(BF16)
    own_low = (own_value - own_high.astype(F32)).astype(BF16)
    own_low_weights = own_weights.astype(BF16)
    own_sum = jnp.dot(own_low_weights, own_high, preferred_element_type=F32)
    own_sum = own_sum + jnp.dot(own_low_weights, own_low, preferred_element_type=F32)

    latent_o[...] = latent_new
    rope_o[...] = rope_new

    pieces = [send_b[me]]
    for off in reversed(order):
        scatter_wait(2, off, send_b, recv_b)
        pieces.append(recv_b[off])
    peaks = [piece[:, 64:65] for piece in pieces]
    highest = own_peak
    for peak in peaks:
        highest = jnp.maximum(highest, peak)
    scale = jnp.exp(own_peak - highest)
    joint_sum = own_sum * scale
    joint_total = own_total * scale
    for piece, peak in zip(pieces, peaks):
        scale = jnp.exp(peak - highest)
        joint_sum = joint_sum + piece * scale
        joint_total = joint_total + piece[:, 96:97] * scale
    values_low = (joint_sum / joint_total).astype(BF16).astype(F32)
    all_b[me] = fold(values_low[0:8], values_low[8:16], low8)
    gather(3, all_b)
    loads[7].wait()
    gather_wait(3, all_b)
    values = jnp.concatenate(
        [unfold_pair(all_b[2 * m], all_b[2 * m + 1], low8) for m in range(n // 2)], 1
    ).astype(BF16)

    proj_s[...] = jnp.dot(values, wo[...], preferred_element_type=F32)
    swap = pltpu.make_async_remote_copy(
        src_ref=proj_s, dst_ref=proj_in, send_sem=tsem.at[0], recv_sem=tsem.at[1],
        device_id=(me, 1 - core), device_id_type=MESH,
    )
    swap.start()
    swap.wait()
    projected = proj_s[...] + proj_in[...]
    squares = jnp.sum(projected * projected, -1, keepdims=True)
    on_diagonal = row == lane
    sq_all[me] = jnp.sum(jnp.where(on_diagonal, squares, 0.0), 0, keepdims=True)
    gather(4, sq_all)
    gather_wait(4, sq_all)
    squares = sq_all[0]
    for k in range(1, n):
        squares = squares + sq_all[k]
    squares = jnp.sum(jnp.where(on_diagonal, squares, 0.0), -1, keepdims=True)
    model_width = x_s.shape[1]
    mixed = (projected * lax.rsqrt(squares / model_width + epsilon) * out_gain[...]).astype(BF16)
    for s in range(seqs):
        mixed_o[s] = mixed[s * props : (s + 1) * props, :]
    for phase, send in ((0, send_a), (2, send_b)):
        for off in order:
            copy_to(phase, off, send.at[lax.rem(me + off, n)], send.at[0]).wait_send()
    for phase, table in ((1, all_a), (3, all_b), (4, sq_all)):
        for off in order:
            copy_to(phase, off, table.at[me], table.at[me]).wait_send()


def finish_kernel(
    seqs, props, shard_len, width,
    lengths, accepted, mixed_h, latent_h, rope_h, rope_in_h, cache_h,
    mixed_o, rope_o, latent_o, cache, out_lat, mixed, latent_new, rope_new, rope_in, out_rope, load_sem, store_sem,
):
    me = lax.axis_index("kv")
    rows = seqs * props
    loads = [pltpu.make_async_copy(cache_h.at[s], cache.at[s], load_sem.at[s]) for s in range(seqs)]
    small = [
        pltpu.make_async_copy(src, dst, load_sem.at[seqs + at])
        for at, (src, dst) in enumerate(
            ((rope_h, rope_new), (rope_in_h, rope_in), (latent_h, latent_new), (mixed_h, mixed))
        )
    ]
    for load in small + loads:
        load.start()
    slot = lane_of((shard_len, rows))
    chosen = []
    small[0].wait()
    small[1].wait()
    for s in range(seqs):
        start = lengths[s] + accepted[s] - me * shard_len
        offset = row_of((shard_len, rows)) - start
        chosen.append(((slot // props == s) & (offset == lax.rem(slot, props))).astype(F32).astype(BF16))
        put_rope = lax.dot_general(rope_new[...], chosen[s], TN, preferred_element_type=F32)[0:ROPE]
        across = lane_of((ROPE, shard_len)) - start
        out_rope[s] = jnp.where((across >= 0) & (across < props), put_rope, rope_in[s].astype(F32)).astype(BF16)
    small[2].wait()
    small[3].wait()
    stores = [
        pltpu.make_async_copy(out_rope, rope_o, store_sem.at[seqs]),
        pltpu.make_async_copy(mixed, mixed_o, store_sem.at[seqs + 1]),
    ]
    for store in stores:
        store.start()
    for s in range(seqs):
        put = jnp.dot(chosen[s], latent_new[...], preferred_element_type=F32)
        down = row_of((shard_len, width)) - (lengths[s] + accepted[s] - me * shard_len)
        loads[s].wait()
        out_lat[s] = jnp.where((down >= 0) & (down < props), put, cache[s].astype(F32)).astype(BF16)
        store = pltpu.make_async_copy(out_lat.at[s], latent_o.at[s], store_sem.at[s])
        store.start()
        stores.append(store)
    for store in stores:
        store.wait()


def fused(
    n, tokens, parents, lengths, accepted, in_gain, w_query, w_latent, w_rope_key, latent_gain, query_gain,
    key_gain, w_key_up, w_value_up, w_out, out_gain, cache_latent, cache_rope,
):
    seqs, props, model_width = tokens.shape
    shard_len, width = cache_latent.shape[1:]
    rows = seqs * props
    places = seqs * shard_len
    heads_wide = w_value_up.shape[1]
    out_cols = w_out.shape[1]
    half = ROPE // 2
    wave = rope_base ** (-np.arange(half, dtype=np.float32) / np.float32(half))
    inverse = np.zeros((1, LANES), np.float32)
    inverse[0, NOPE : NOPE + half] = wave
    inverse[0, NOPE + half : QK] = wave
    smem = pl.BlockSpec(memory_space=pltpu.SMEM)
    vmem = pl.BlockSpec(memory_space=pltpu.VMEM)
    hbm = pl.BlockSpec(memory_space=pl.ANY)
    rope_in = jnp.swapaxes(cache_rope, 1, 2)
    held = [w_query, w_latent, w_rope_key.T, w_key_up, w_value_up, w_out, cache_latent, rope_in]
    mixed, latent_new, rope_new = pl.pallas_call(
        functools.partial(fused_kernel, n, seqs, props, shard_len, width),
        out_shape=(
            jax.ShapeDtypeStruct((seqs, props, out_cols), BF16),
            jax.ShapeDtypeStruct((rows, width), BF16),
            jax.ShapeDtypeStruct((rows, LANES), BF16),
        ),
        in_specs=[smem] * 3 + [vmem] * 7 + [hbm] * 8,
        out_specs=(vmem, vmem, vmem),
        scratch_shapes=[pltpu.VMEM(array.shape, array.dtype) for array in held]
        + [
            pltpu.VMEM((rows, model_width), F32),
            pltpu.VMEM((rows, model_width), BF16),
            pltpu.VMEM((n // 4, 4 * QK, places), BF16),
            pltpu.VMEM((places, heads_wide), BF16),
            pltpu.VMEM((places, heads_wide), BF16),
            pltpu.VMEM((n, rows, LANES), F32),
            pltpu.VMEM((n, rows, LANES), F32),
            pltpu.VMEM((n, rows, LANES), F32),
            pltpu.VMEM((n, rows, LANES), F32),
            pltpu.VMEM((n, rows, LANES), F32),
            pltpu.VMEM((n, 8, LANES), F32),
            pltpu.VMEM((rows, out_cols), F32),
            pltpu.VMEM((rows, out_cols), F32),
            pltpu.VMEM((n, 1, LANES), F32),
            pltpu.VMEM((2, rows // 2, width), F32),
            pltpu.SemaphoreType.DMA((len(held),)),
            pltpu.SemaphoreType.DMA((5, n)),
            pltpu.SemaphoreType.DMA((5, n)),
            pltpu.SemaphoreType.DMA((4,)),
        ],
        compiler_params=pltpu.CompilerParams(
            collective_id=0, has_side_effects=True, vmem_limit_bytes=56 * 1024 * 1024
        ),
    )(
        parents, lengths, accepted, tokens, in_gain.reshape(1, -1), latent_gain.reshape(1, -1),
        query_gain.reshape(1, -1), key_gain.reshape(1, -1), out_gain.reshape(1, -1), jnp.asarray(inverse), *held,
    )
    mixed, new_rope, new_latent = pl.pallas_call(
        functools.partial(finish_kernel, seqs, props, shard_len, width),
        out_shape=(
            jax.ShapeDtypeStruct(mixed.shape, BF16),
            jax.ShapeDtypeStruct(rope_in.shape, BF16),
            jax.ShapeDtypeStruct(cache_latent.shape, BF16),
        ),
        in_specs=[smem] * 2 + [hbm] * 5,
        out_specs=(hbm, hbm, hbm),
        scratch_shapes=[
            pltpu.VMEM(cache_latent.shape, BF16),
            pltpu.VMEM(cache_latent.shape, BF16),
            pltpu.VMEM(mixed.shape, BF16),
            pltpu.VMEM(latent_new.shape, BF16),
            pltpu.VMEM(rope_new.shape, BF16),
            pltpu.VMEM(rope_in.shape, BF16),
            pltpu.VMEM(rope_in.shape, BF16),
            pltpu.SemaphoreType.DMA((seqs + 4,)),
            pltpu.SemaphoreType.DMA((seqs + 2,)),
        ],
    )(lengths, accepted, mixed, latent_new, rope_new, rope_in, cache_latent)
    return mixed, new_latent, jnp.swapaxes(new_rope, 1, 2)


def step(n, cores, tokens, *others):
    w_query, w_latent, w_key_up, cache_latent = others[4], others[5], others[10], others[14]
    fits = (
        tokens.shape[0] * tokens.shape[1] == 16
        and cores == 2
        and w_key_up.shape[1] == n * NOPE
        and w_latent.shape[1] == n * 64
        and n % 4 == 0
        and w_query.shape[0] % LANES == 0
        and cache_latent.shape[1] == LANES
    )
    if fits:
        return fused(n, tokens, *others)
    return body(tokens, *others)


def solution(mesh):
    return jax.shard_map(
        functools.partial(step, mesh.shape["kv"], mesh.shape["tp"]),
        mesh=mesh,
        in_specs=(
            P(),
            P(),
            P(),
            P(),
            P(),
            P("kv", "tp"),
            P("kv", None),
            P(),
            P(),
            P(),
            P(),
            P(None, "tp"),
            P(None, "tp"),
            P("tp", "kv"),
            P("kv"),
            P(None, "kv", None),
            P(None, "kv", None),
        ),
        out_specs=(P(None, None, "kv"), P(None, "kv", None), P(None, "kv", None)),
        check_vma=False,
    )
```
